32 devices in a mesh: sp: 4 (over z), fs: 4 (over y, x), tp: 2 (over core).
Axes of the slice: x: 2, y: 2, z: 4, core: 2. Of those that a mesh axis runs over, the one named last changes fastest.
Arguments:
- tokens: bfloat16 [4, 512, 2048], P('fs', 'sp'), may hold values from -6 to 6
- norm_gain: float32 [2048], replicated, may hold values from 0.1 to 1.9
- w_ret_query: bfloat16 [2048, 2048], P(('sp', 'fs'), 'tp'), may hold values from -0.125 to 0.125
- w_ret_key: bfloat16 [2048, 2048], P(('sp', 'fs'), 'tp'), may hold values from -0.125 to 0.125
- w_ret_value: bfloat16 [2048, 2048], P(('sp', 'fs'), 'tp'), may hold values from -0.125 to 0.125
- w_q_down: bfloat16 [2048, 768], P(('sp', 'fs'), 'tp'), may hold values from -0.125 to 0.125
- w_kv_down: bfloat16 [2048, 512], P(('sp', 'fs'), 'tp'), may hold values from -0.125 to 0.125
- w_rope_key: bfloat16 [2048, 64], P(('sp', 'fs')), may hold values from -0.125 to 0.125
- w_q_up: bfloat16 [768, 3072], P(None, 'tp'), may hold values from -0.21875 to 0.21875
- w_kv_up: bfloat16 [512, 4096], P(None, 'tp'), may hold values from -0.25 to 0.25
- q_lat_gain: float32 [768], replicated, may hold values from 0.4 to 10
- kv_lat_gain: float32 [512], replicated, may hold values from 0.4 to 10
- att_norm_gain: float32 [2048], P('tp'), may hold values from 0.1 to 1.9
- ret_norm_gain: float32 [2048], P('tp'), may hold values from 0.1 to 1.9
- w_ret_out: bfloat16 [2048, 2048], P(('sp', 'fs'), 'tp'), may hold values from -0.09375 to 0.09375
- w_att_out: bfloat16 [2048, 2048], P(('sp', 'fs'), 'tp'), may hold values from -0.09375 to 0.09375
- head_rate: float32 [8], P('tp'), may hold values from -0.05 to 0
- decay_shift: float32 [4, 8, 512], P('fs', 'tp', 'sp'), may hold values from -1.1 to 0
- start_state: float32 [4, 8, 256, 256], P('fs', 'tp'), may hold values from -20 to 20
Outputs:
- mixed: bfloat16 [4, 512, 2048], P('fs', ('sp', 'tp'))
The draws below stay inside these ranges and needn't reach their ends.
All inputs are finite; a program needn't handle non-finite values.
Results may differ from the reference program's by a relative error of at most 0.018.
The reference program's roundings to bfloat16 on the way count: a program that leaves them out, or rounds other values in their place, can miss the bound.
Values may be sent and summed in bfloat16 or wider, within the bound.
A program may use at most 64 MiB of HBM per device.

```python
import jax
import jax.numpy as jnp
from jax import lax

D = 2048
RETENTION_HEADS = 8
RET_DIM = 256
ATT_HEADS = 16
NOPE_DIM = 128
ROPE_DIM = 64
VAL_DIM = 128
Q_LAT = 768
KV_LAT = 512
TOK_DEV = 128
SEQUENCE_LENGTH = 512
SEQUENCE_COUNT = 4
N_SP = 4
N_TP = 2


def draw_head_rate(key, part):
    key_perm, key_fast, key_slow = jax.random.split(key, 3)
    shuffled = jax.random.permutation(key_perm, RETENTION_HEADS)
    quick_count = RETENTION_HEADS // 2
    is_fast = shuffled < quick_count
    fast_rate = jnp.exp(jax.random.uniform(key_fast, (RETENTION_HEADS,), jnp.float32, jnp.log(0.02), jnp.log(0.05)))
    slow_rate = jnp.exp(jax.random.uniform(key_slow, (RETENTION_HEADS,), jnp.float32, jnp.log(0.05), jnp.log(0.5))) / SEQUENCE_LENGTH
    return -jnp.where(is_fast, fast_rate, slow_rate)


def draw_decay_shift(key, part):
    key_block, key_jitter, key_offsets, key_decay_factor = jax.random.split(key, 4)
    blocks = SEQUENCE_LENGTH // TOK_DEV
    block_level = jax.random.uniform(key_block, (SEQUENCE_COUNT, RETENTION_HEADS, blocks, 1), jnp.float32, 0.1, 0.6)
    jitter = jax.random.uniform(key_jitter, (SEQUENCE_COUNT, RETENTION_HEADS, blocks, TOK_DEV), jnp.float32, 0.5, 1.5)
    constant_decay = -(block_level * jitter).reshape(SEQUENCE_COUNT, RETENTION_HEADS, SEQUENCE_LENGTH) / SEQUENCE_LENGTH
    segment_index = jax.random.randint(key_offsets, (SEQUENCE_COUNT, RETENTION_HEADS, 2), 0, SEQUENCE_LENGTH)
    segment_length = jax.random.uniform(key_decay_factor, (SEQUENCE_COUNT, RETENTION_HEADS, 2), jnp.float32, 0.22, 0.5)
    position_offsets = jnp.arange(SEQUENCE_LENGTH)[None, None, None, :] == segment_index[..., None]
    segment_count = jnp.sum(jnp.where(position_offsets, segment_length[..., None], 0.0), axis=2)
    return constant_decay - segment_count


def draw_q_lat_gain(key, part):
    return jnp.clip(1.0 + 0.18 * jax.random.normal(key, (Q_LAT,), jnp.float32), 0.4, 1.6)


def draw_kv_lat_gain(key, part):
    return jnp.clip(1.0 + 0.18 * jax.random.normal(key, (KV_LAT,), jnp.float32), 0.4, 1.6)


def shard_levels(stream_key, shape, shards, least, high):
    factor_of, own = 1.0, jax.random.fold_in(stream_key, 6)
    for axis_at, shards_of in shards:
        draws = jnp.exp(jax.random.uniform(jax.random.fold_in(own, axis_at), (shards_of,), jnp.float32, least / len(shards), high / len(shards)))
        factor_of = factor_of * jnp.repeat(draws, shape[axis_at] // shards_of).reshape([-1 if axis == axis_at else 1 for axis in range(len(shape))])
    return factor_of


def noise(own_key, dims, scale, reach, shards=(), kind=jnp.bfloat16):
    gain = shard_levels(own_key, dims, shards, -0.22, 0.18) if shards else 1.0
    array = jax.random.normal(own_key, dims, jnp.float32) * scale * gain
    return jnp.minimum(jnp.maximum(array, -reach), reach).astype(kind)


def setup_inputs(seed: int = 0) -> dict:
    seeds = jax.random.split(jax.random.key(seed), 20)
    return {
        "tokens": noise(seeds[0], (SEQUENCE_COUNT, SEQUENCE_LENGTH, D), 1.0, 6.0, ((0, 4), (1, 4))),
        "norm_gain": jnp.clip(1.0 + 0.18 * jax.random.normal(seeds[1], (D,), jnp.float32), 0.1, 1.9),
        "w_ret_query": noise(seeds[2], (D, RETENTION_HEADS * RET_DIM), D ** -0.5, 0.125, ((0, 16), (1, 2))),
        "w_ret_key": noise(seeds[3], (D, RETENTION_HEADS * RET_DIM), D ** -0.5, 0.125, ((0, 16), (1, 2))),
        "w_ret_value": noise(seeds[4], (D, RETENTION_HEADS * RET_DIM), D ** -0.5, 0.125, ((0, 16), (1, 2))),
        "w_q_down": noise(seeds[5], (D, Q_LAT), D ** -0.5, 0.125, ((0, 16), (1, 2))),
        "w_kv_down": noise(seeds[6], (D, KV_LAT), D ** -0.5, 0.125, ((0, 16), (1, 2))),
        "w_rope_key": noise(seeds[7], (D, ROPE_DIM), D ** -0.5, 0.125, ((0, 16),)),
        "w_q_up": noise(seeds[8], (Q_LAT, ATT_HEADS * (NOPE_DIM + ROPE_DIM)), Q_LAT ** -0.5, 0.21875, ((1, 2),)),
        "w_kv_up": noise(seeds[9], (KV_LAT, ATT_HEADS * (NOPE_DIM + VAL_DIM)), KV_LAT ** -0.5, 0.25, ((1, 2),)),
        "q_lat_gain": draw_q_lat_gain(jax.random.fold_in(seeds[19], 71), 0),
        "kv_lat_gain": draw_kv_lat_gain(jax.random.fold_in(seeds[19], 71), 0),
        "att_norm_gain": jnp.clip(1.0 + 0.18 * jax.random.normal(seeds[12], (ATT_HEADS * VAL_DIM,), jnp.float32), 0.1, 1.9),
        "ret_norm_gain": jnp.clip(1.0 + 0.18 * jax.random.normal(seeds[13], (RETENTION_HEADS * RET_DIM,), jnp.float32), 0.1, 1.9),
        "w_ret_out": noise(seeds[14], (D, RETENTION_HEADS * RET_DIM), (RETENTION_HEADS * RET_DIM + ATT_HEADS * VAL_DIM) ** -0.5, 0.09375, ((0, 16), (1, 2))),
        "w_att_out": noise(seeds[15], (D, ATT_HEADS * VAL_DIM), (RETENTION_HEADS * RET_DIM + ATT_HEADS * VAL_DIM) ** -0.5, 0.09375, ((0, 16), (1, 2))),
        "head_rate": draw_head_rate(jax.random.fold_in(seeds[19], 71), 0),
        "decay_shift": draw_decay_shift(jax.random.fold_in(seeds[19], 71), 0),
        "start_state": noise(seeds[18], (SEQUENCE_COUNT, RETENTION_HEADS, RET_DIM, RET_DIM), (0.15 * (TOK_DEV * N_SP) ** 0.5), 20.0, ((0, 4), (1, 2)), jnp.float32),
    }


EPSILON = 1e-06
THETA_BASE = 10000.0
TOP_PRECISION = lax.Precision.HIGHEST

def angle_tables(positions, rot_width):
    half_width = rot_width // 2
    inverse = THETA_BASE ** (-jnp.arange(half_width, dtype=jnp.float32) * 2.0 / rot_width)
    angles = positions.astype(jnp.float32)[:, None] * inverse[None, :]
    return (jnp.cos(angles), jnp.sin(angles))

def rotate(values, cosine, sine):
    half_width = values.shape[-1] // 2
    front_half = values[..., :half_width]
    back_half = values[..., half_width:]
    return jnp.concatenate([front_half * cosine - back_half * sine, back_half * cosine + front_half * sine], axis=-1)

def rms_scale(values, gain_vector):
    return values * lax.rsqrt(lax.optimization_barrier(jnp.mean(values * values, axis=-1, keepdims=True)) + EPSILON) * gain_vector

def saved_states(values):
    return lax.optimization_barrier(values.astype(jnp.bfloat16))

def reference(tokens, norm_gain, w_ret_query, w_ret_key, w_ret_value, w_q_down, w_kv_down, w_rope_key, w_q_up, w_kv_up, q_lat_gain, kv_lat_gain, att_norm_gain, ret_norm_gain, w_ret_out, w_att_out, head_rate, decay_shift, start_state):
    positions = jnp.arange(SEQUENCE_LENGTH, dtype=jnp.int32)
    ret_cos, ret_sin = angle_tables(positions, RET_DIM)
    rope_cos, rope_sin = angle_tables(positions, ROPE_DIM)
    att_scale = (NOPE_DIM + ROPE_DIM) ** (-0.5)
    group_ret = RETENTION_HEADS * RET_DIM // N_TP
    group_att = ATT_HEADS * VAL_DIM // N_TP

    def one_sequence(inputs):
        sequence, shift_rows, first_state = inputs
        source = sequence.astype(jnp.float32)
        normed = saved_states(rms_scale(source, norm_gain))

        def project(weight):
            return jnp.dot(normed, weight, preferred_element_type=jnp.float32)
        retention_query = saved_states(rotate(project(w_ret_query).reshape(SEQUENCE_LENGTH, RETENTION_HEADS, RET_DIM), ret_cos[:, None], ret_sin[:, None]))
        retention_key = saved_states(rotate(project(w_ret_key).reshape(SEQUENCE_LENGTH, RETENTION_HEADS, RET_DIM), ret_cos[:, None], ret_sin[:, None]) * RET_DIM ** (-0.5))
        retention_value = saved_states(project(w_ret_value).reshape(SEQUENCE_LENGTH, RETENTION_HEADS, RET_DIM))
        lat_q_raw = saved_states(project(w_q_down))
        lat_kv_raw = saved_states(project(w_kv_down))
        rope_key = saved_states(rotate(project(w_rope_key), rope_cos, rope_sin))
        q_latent = saved_states(rms_scale(lat_q_raw.astype(jnp.float32), q_lat_gain))
        kv_latent = saved_states(rms_scale(lat_kv_raw.astype(jnp.float32), kv_lat_gain))
        query_full = jnp.dot(q_latent, w_q_up, preferred_element_type=jnp.float32).reshape(SEQUENCE_LENGTH, ATT_HEADS, NOPE_DIM + ROPE_DIM)
        att_query = saved_states(jnp.concatenate([query_full[..., :NOPE_DIM], rotate(query_full[..., NOPE_DIM:], rope_cos[:, None], rope_sin[:, None])], axis=-1))
        expanded = saved_states(jnp.dot(kv_latent, w_kv_up, preferred_element_type=jnp.float32)).reshape(SEQUENCE_LENGTH, ATT_HEADS, NOPE_DIM + VAL_DIM)
        key_nope = expanded[..., :NOPE_DIM].astype(jnp.float32)
        key_values = expanded[..., NOPE_DIM:].astype(jnp.float32)
        rope_wide = rope_key.astype(jnp.float32)

        def query_block(block_index):
            first_row = block_index * TOK_DEV
            block_query = lax.dynamic_slice_in_dim(att_query, first_row, TOK_DEV, 0).astype(jnp.float32)
            score_matrix = (jnp.einsum('qhd,khd->hqk', block_query[..., :NOPE_DIM], key_nope) + jnp.einsum('qhd,kd->hqk', block_query[..., NOPE_DIM:], rope_wide)) * att_scale
            allowed = positions[None, :] <= (first_row + jnp.arange(TOK_DEV, dtype=jnp.int32))[:, None]
            masked = jnp.where(allowed[None], score_matrix, -jnp.inf)
            weights = jnp.exp(masked - lax.optimization_barrier(jnp.max(masked, axis=-1, keepdims=True)))
            rounded = saved_states(weights).astype(jnp.float32)
            numerator = jnp.einsum('hqk,khd->qhd', rounded, key_values)
            denominator = lax.optimization_barrier(jnp.sum(weights, axis=-1))
            return numerator / denominator.T[:, :, None]
        att_raw = lax.map(query_block, jnp.arange(N_SP)).reshape(SEQUENCE_LENGTH, ATT_HEADS, VAL_DIM)
        att_out = saved_states(rms_scale(att_raw, att_norm_gain.reshape(ATT_HEADS, VAL_DIM))).reshape(SEQUENCE_LENGTH, ATT_HEADS * VAL_DIM)
        log_rates = head_rate[:, None] + shift_rows
        offsets = jnp.arange(TOK_DEV, dtype=jnp.int32)
        lower_mask = offsets[None, :] <= offsets[:, None]

        def ret_block(carried_state, block_index):
            first_row = block_index * TOK_DEV
            cumul = jnp.cumsum(lax.dynamic_slice_in_dim(log_rates, first_row, TOK_DEV, 1), axis=1)
            decay_matrix = jnp.exp(jnp.where(lower_mask[None], cumul[:, :, None] - cumul[:, None, :], -jnp.inf))
            block_queries = lax.dynamic_slice_in_dim(retention_query, first_row, TOK_DEV, 0).astype(jnp.float32)
            block_keys = lax.dynamic_slice_in_dim(retention_key, first_row, TOK_DEV, 0).astype(jnp.float32)
            block_values = lax.dynamic_slice_in_dim(retention_value, first_row, TOK_DEV, 0).astype(jnp.float32)
            score_matrix = saved_states(jnp.einsum('zgq,ugq->gzu', block_queries, block_keys) * decay_matrix).astype(jnp.float32)
            inside_block_output = jnp.einsum('vzs,svp->zvp', score_matrix, block_values)
            carried_term = jnp.einsum('nhd,hde->nhe', block_queries, carried_state, precision=TOP_PRECISION) * jnp.exp(cumul).T[:, :, None]
            block_output_sum = cumul[:, -1]
            weighted_values = block_keys * jnp.exp(block_output_sum[:, None] - cumul).T[:, :, None]
            updated_state = jnp.exp(block_output_sum)[:, None, None] * carried_state + jnp.einsum('uzj,uzv->zjv', weighted_values, block_values, precision=TOP_PRECISION)
            return (updated_state, inside_block_output + carried_term)
        ignored_state, ret_blocks = lax.scan(ret_block, first_state, jnp.arange(N_SP))
        ret_raw = ret_blocks.reshape(SEQUENCE_LENGTH, RETENTION_HEADS, RET_DIM)
        row_mean = lax.optimization_barrier(jnp.mean(ret_raw, axis=-1, keepdims=True))
        centered = ret_raw - row_mean
        row_var = lax.optimization_barrier(jnp.mean(centered * centered, axis=-1, keepdims=True))
        ret_out = saved_states(centered * lax.rsqrt(row_var + EPSILON) * ret_norm_gain.reshape(RETENTION_HEADS, RET_DIM)).reshape(SEQUENCE_LENGTH, RETENTION_HEADS * RET_DIM)
        summed = jnp.zeros((SEQUENCE_LENGTH, D), jnp.float32)
        for group_index in range(N_TP):
            ret_cols = slice(group_index * group_ret, (group_index + 1) * group_ret)
            att_cols = slice(group_index * group_att, (group_index + 1) * group_att)
            partial_value = jnp.dot(ret_out[:, ret_cols], w_ret_out[:, ret_cols].T, preferred_element_type=jnp.float32) + jnp.dot(att_out[:, att_cols], w_att_out[:, att_cols].T, preferred_element_type=jnp.float32)
            summed = summed + saved_states(partial_value).astype(jnp.float32)
        return summed.astype(jnp.bfloat16)
    return lax.map(one_sequence, (tokens, decay_shift, start_state))
```

```python
import functools

import jax
import jax.numpy as jnp
from jax import lax
from jax.experimental import pallas as pl
from jax.experimental.pallas import tpu as pltpu
from jax.sharding import PartitionSpec as P

RET_DIM = 256
NOPE_DIM = 128
ROPE_DIM = 64
VAL_DIM = 128
KV_LAT = 512


EPSILON = 1e-06
THETA_BASE = 10000.0
TOP_PRECISION = lax.Precision.HIGHEST


def prefix(x, axis, combine, identity):
    peers, position = (lax.axis_size(axis), lax.axis_index(axis))
    everything = jax.tree.map(
        lambda part, kind: lax.all_gather(part.astype(kind), axis), x, (jnp.bfloat16, jnp.bfloat16)
    )
    start = jax.tree.map(
        lambda part, zero: jnp.broadcast_to(jnp.asarray(zero, part.dtype), part.shape), x, identity
    )

    def lap(k, before):
        reached = k < position
        new = combine(
            before, jax.tree.map(lambda part, own: part[k].astype(own.dtype), everything, x)
        )
        return jax.tree.map(lambda a, b: jnp.where(reached, a, b), new, before)

    return lax.fori_loop(0, peers, lap, start)


def angle_tables(positions, rot_width):
    half_width = rot_width // 2
    inverse = THETA_BASE ** (-jnp.arange(half_width, dtype=jnp.float32) * 2.0 / rot_width)
    angles = positions.astype(jnp.float32)[:, None] * inverse[None, :]
    return (jnp.cos(angles), jnp.sin(angles))


def rotate(values, cosine, sine):
    half_width = values.shape[-1] // 2
    front_half = values[..., :half_width]
    back_half = values[..., half_width:]
    return jnp.concatenate(
        [front_half * cosine - back_half * sine, back_half * cosine + front_half * sine], axis=-1
    )


def rms_scale(values, gain_vector):
    return (
        values
        * lax.rsqrt(jnp.mean(values * values, axis=-1, keepdims=True) + EPSILON)
        * gain_vector
    )


def chain_states(earlier, later):
    early_log, early_state = earlier
    late_log, late_state = later
    return (early_log + late_log, jnp.exp(late_log)[:, None, None] * early_state + late_state)


def rows_plan(
    tokens,
    norm_gain,
    w_ret_query,
    w_ret_key,
    w_ret_value,
    w_q_down,
    w_kv_down,
    w_rope_key,
    w_q_up,
    w_kv_up,
    q_lat_gain,
    kv_lat_gain,
    att_norm_gain,
    ret_norm_gain,
    w_ret_out,
    w_att_out,
    head_rate,
    decay_shift,
    start_state,
):
    tok_rows = tokens.shape[1]
    ret_local = head_rate.shape[0]
    att_local = w_q_up.shape[1] // (NOPE_DIM + ROPE_DIM)
    row_offset = lax.axis_index("sp") * tok_rows
    positions = row_offset + jnp.arange(tok_rows, dtype=jnp.int32)
    (
        full_query,
        full_key,
        full_value,
        full_q_down,
        full_kv_down,
        full_rope,
        full_ret_out,
        full_att_out,
    ) = (
        lax.all_gather(w_ret_query, ("sp", "fs"), axis=0, tiled=True),
        lax.all_gather(w_ret_key, ("sp", "fs"), axis=0, tiled=True),
        lax.all_gather(w_ret_value, ("sp", "fs"), axis=0, tiled=True),
        lax.all_gather(w_q_down, ("sp", "fs"), axis=0, tiled=True),
        lax.all_gather(w_kv_down, ("sp", "fs"), axis=0, tiled=True),
        lax.all_gather(w_rope_key, ("sp", "fs"), axis=0, tiled=True),
        lax.all_gather(w_ret_out, ("sp", "fs"), axis=0, tiled=True),
        lax.all_gather(w_att_out, ("sp", "fs"), axis=0, tiled=True),
    )
    source = tokens[0].astype(jnp.float32)
    normed = rms_scale(source, norm_gain).astype(jnp.bfloat16)
    ret_cos, ret_sin = angle_tables(positions, RET_DIM)
    rope_cos, rope_sin = angle_tables(positions, ROPE_DIM)

    def project(weight):
        return jnp.dot(normed, weight, preferred_element_type=jnp.float32)

    part_q = project(full_q_down).astype(jnp.bfloat16)
    part_kv = project(full_kv_down).astype(jnp.bfloat16)
    lat_q_raw, lat_kv_raw = (
        lax.all_gather(part_q, "tp", axis=1, tiled=True),
        lax.all_gather(part_kv, "tp", axis=1, tiled=True),
    )
    retention_query = rotate(
        project(full_query).reshape(tok_rows, ret_local, RET_DIM),
        ret_cos[:, None],
        ret_sin[:, None],
    ).astype(jnp.bfloat16)
    retention_key = (
        rotate(
            project(full_key).reshape(tok_rows, ret_local, RET_DIM),
            ret_cos[:, None],
            ret_sin[:, None],
        )
        * RET_DIM ** (-0.5)
    ).astype(jnp.bfloat16)
    retention_value = project(full_value).reshape(tok_rows, ret_local, RET_DIM).astype(jnp.bfloat16)
    rope_key = rotate(project(full_rope), rope_cos, rope_sin).astype(jnp.bfloat16)
    log_rates = head_rate[:, None] + decay_shift[0]
    cumul = jnp.cumsum(log_rates, axis=1)
    offsets = jnp.arange(tok_rows, dtype=jnp.int32)
    lower_mask = offsets[None, :] <= offsets[:, None]
    decay_matrix = jnp.exp(
        jnp.where(lower_mask[None], cumul[:, :, None] - cumul[:, None, :], -jnp.inf)
    )
    block_score_grid = (
        jnp.einsum(
            "zgq,ugq->gzu", retention_query, retention_key, preferred_element_type=jnp.float32
        )
        * decay_matrix
    ).astype(jnp.bfloat16)
    inside_block_output = jnp.einsum(
        "vzs,svp->zvp", block_score_grid, retention_value, preferred_element_type=jnp.float32
    )
    block_output_sum = cumul[:, -1]
    weighted_values = (
        retention_key.astype(jnp.float32) * jnp.exp(block_output_sum[:, None] - cumul).T[:, :, None]
    )
    contribution = jnp.einsum(
        "uzj,uzv->zjv",
        weighted_values,
        retention_value.astype(jnp.float32),
        precision=TOP_PRECISION,
    )
    identity = (jnp.zeros_like(block_output_sum), jnp.zeros_like(contribution))
    before_log, before_state = prefix(
        (block_output_sum, contribution), "sp", chain_states, identity
    )
    q_latent = rms_scale(lat_q_raw.astype(jnp.float32), q_lat_gain).astype(jnp.bfloat16)
    kv_latent = rms_scale(lat_kv_raw.astype(jnp.float32), kv_lat_gain).astype(jnp.bfloat16)
    query_full = jnp.dot(q_latent, w_q_up, preferred_element_type=jnp.float32).reshape(
        tok_rows, att_local, NOPE_DIM + ROPE_DIM
    )
    query_nope = query_full[..., :NOPE_DIM].astype(jnp.bfloat16)
    query_rope = rotate(query_full[..., NOPE_DIM:], rope_cos[:, None], rope_sin[:, None]).astype(
        jnp.bfloat16
    )
    att_scale = (NOPE_DIM + ROPE_DIM) ** (-0.5)

    def attend(carry, key_nope, key_values, key_rope, start):
        running_max, running_sum, running_acc = carry
        key_count = key_rope.shape[0]
        score_matrix = (
            jnp.einsum("qhd,khd->hqk", query_nope, key_nope, preferred_element_type=jnp.float32)
            + jnp.einsum("qhd,kd->hqk", query_rope, key_rope, preferred_element_type=jnp.float32)
        ) * att_scale
        key_positions = start + jnp.arange(key_count, dtype=jnp.int32)
        allowed = key_positions[None, :] <= positions[:, None]
        masked = jnp.where(allowed[None], score_matrix, -jnp.inf)
        new_max = jnp.maximum(running_max, jnp.max(masked, axis=-1))
        safe_max = jnp.where(jnp.isfinite(new_max), new_max, 0.0)
        weights = jnp.exp(masked - safe_max[..., None])
        rescale = jnp.exp(running_max - safe_max)
        new_sum = running_sum * rescale + jnp.sum(weights, axis=-1)
        new_acc = running_acc * rescale[..., None] + jnp.einsum(
            "hqk,khd->hqd",
            weights.astype(jnp.bfloat16),
            key_values,
            preferred_element_type=jnp.float32,
        )
        return (new_max, new_sum, new_acc)

    def expand_attend(carry_in, lat_piece, rope_piece, start):
        wide = (
            jnp.dot(lat_piece, w_kv_up, preferred_element_type=jnp.float32)
            .astype(jnp.bfloat16)
            .reshape(rope_piece.shape[0], att_local, NOPE_DIM + VAL_DIM)
        )
        return attend(carry_in, wide[..., :NOPE_DIM], wide[..., NOPE_DIM:], rope_piece, start)

    empty = (
        jnp.full((att_local, tok_rows), -jnp.inf, jnp.float32),
        jnp.zeros((att_local, tok_rows), jnp.float32),
        jnp.zeros((att_local, tok_rows, VAL_DIM), jnp.float32),
    )
    groups = lax.axis_size("tp")
    kv_part = KV_LAT // groups
    rope_part = ROPE_DIM // groups
    my_group = lax.axis_index("tp")
    joined = jnp.concatenate(
        [
            lax.dynamic_slice_in_dim(kv_latent, my_group * kv_part, kv_part, 1),
            lax.dynamic_slice_in_dim(rope_key, my_group * rope_part, rope_part, 1),
        ],
        axis=1,
    )
    all_rows = lax.all_gather(joined, "sp", axis=0, tiled=True)
    complete = lax.all_gather(all_rows, "tp", axis=1, tiled=True)
    total_rows = complete.shape[0]
    grouped = complete.reshape(total_rows, groups, kv_part + rope_part)
    lat_all = grouped[:, :, :kv_part].reshape(total_rows, KV_LAT)
    rope_all = grouped[:, :, kv_part:].reshape(total_rows, ROPE_DIM)

    def visit(block_index, carry_in):
        start = block_index * tok_rows
        lat_piece = lax.dynamic_slice_in_dim(lat_all, start, tok_rows, 0)
        rope_piece = lax.dynamic_slice_in_dim(rope_all, start, tok_rows, 0)
        return expand_attend(carry_in, lat_piece, rope_piece, start)

    final = lax.fori_loop(0, lax.axis_index("sp") + 1, visit, empty)
    att_raw = jnp.transpose(final[2] / final[1][..., None], (1, 0, 2))
    att_out = (
        rms_scale(att_raw, att_norm_gain.reshape(att_local, VAL_DIM))
        .astype(jnp.bfloat16)
        .reshape(tok_rows, att_local * VAL_DIM)
    )
    entering = jnp.exp(before_log)[:, None, None] * start_state[0] + before_state
    carried_term = (
        jnp.einsum(
            "nhd,hde->nhe", retention_query.astype(jnp.float32), entering, precision=TOP_PRECISION
        )
        * jnp.exp(cumul).T[:, :, None]
    )
    ret_raw = inside_block_output + carried_term
    row_mean = jnp.mean(ret_raw, axis=-1, keepdims=True)
    centered = ret_raw - row_mean
    row_var = jnp.mean(centered * centered, axis=-1, keepdims=True)
    ret_out = (
        (centered * lax.rsqrt(row_var + EPSILON) * ret_norm_gain.reshape(ret_local, RET_DIM))
        .astype(jnp.bfloat16)
        .reshape(tok_rows, ret_local * RET_DIM)
    )
    contract = (((1,), (1,)), ((), ()))
    mixed = lax.psum_scatter(
        (
            lax.dot_general(ret_out, full_ret_out, contract, preferred_element_type=jnp.float32)
            + lax.dot_general(att_out, full_att_out, contract, preferred_element_type=jnp.float32)
        ).astype(jnp.bfloat16),
        "tp",
        scatter_dimension=0,
        tiled=True,
    )
    return mixed[None]


MESH = pl.DeviceIdType.MESH


def heads_fit(mesh, ret_local, sequences):
    sizes = mesh.shape
    return (
        sizes["fs"] == 4 and sizes["tp"] == 2 and ret_local == sizes["sp"] and sequences == 1
    )


def gather_kernel(
    n_sp,
    tok_ref,
    lat_ref,
    wq_ref,
    wk_ref,
    wv_ref,
    wr_ref,
    wa_ref,
    shift_ref,
    tok_all,
    w_all,
    shift_all,
    local_sem,
    z_send,
    z_recv,
    x_send,
    x_recv,
    y_send,
    y_recv,
    xf_send,
    xf_recv,
    yf_send,
    yf_recv,
    t_send,
    t_recv,
    p_send,
    p_recv,
    s_send,
    s_recv,
):
    z, f, t = lax.axis_index("sp"), lax.axis_index("fs"), lax.axis_index("tp")
    xn = f + 1 - 2 * (f % 2)
    yn = (f + 2) % 4
    other = 1 - t
    rows = tok_ref.shape[0]
    half = rows // 2
    wide = lat_ref.shape[2]
    group = 3 * wide
    fs = 4
    weights = (lat_ref, wq_ref, wk_ref, wv_ref, wr_ref, wa_ref)

    def remote(src, dst, send, recv, **where):
        return pltpu.make_async_remote_copy(
            src_ref=src,
            dst_ref=dst,
            send_sem=send,
            recv_sem=recv,
            device_id={"sp": z, "fs": f, "tp": t, **where},
            device_id_type=MESH,
        )

    barrier = pltpu.get_barrier_semaphore()
    peers = [{"sp": (z + d) % n_sp, "fs": f, "tp": t} for d in range(1, n_sp)]
    peers += [{"sp": z, "fs": xn, "tp": t}, {"sp": z, "fs": yn, "tp": t}]
    peers += [{"sp": z, "fs": f, "tp": other}]
    for peer in peers:
        pl.semaphore_signal(barrier, inc=1, device_id=peer, device_id_type=MESH)
    pl.semaphore_wait(barrier, len(peers))

    def piece(u, owner):
        if u == 0:
            return lat_ref.at[owner]
        return weights[u].at[:, pl.ds(pl.multiple_of(owner * wide, wide), wide)]

    def block(owner):
        return pl.ds(pl.multiple_of((owner * fs + f) * rows, rows), rows)

    pending = []
    mine = pl.ds(pl.multiple_of(t * half, half), half)
    tok_copies = {}
    for d in range(1, n_sp):
        copy = remote(
            tok_ref.at[mine],
            tok_all.at[z, mine],
            t_send.at[d],
            t_recv.at[d],
            sp=(z + d) % n_sp,
        )
        copy.start()
        tok_copies[d] = copy
        copy = remote(
            shift_ref, shift_all.at[z], s_send.at[d], s_recv.at[d], sp=(z + d) % n_sp
        )
        copy.start()
        pending.append(copy)
    locals_ = []
    for u in range(6):
        copy = pltpu.make_async_copy(
            piece(u, z), w_all.at[block(z), pl.ds(u * wide, wide)], local_sem.at[u]
        )
        copy.start()
        locals_.append(copy)
    own_tok = pltpu.make_async_copy(tok_ref, tok_all.at[z], local_sem.at[6])
    own_tok.start()
    own_shift = pltpu.make_async_copy(shift_ref, shift_all.at[z], local_sem.at[7])
    own_shift.start()
    z_copies = {}
    for g in range(2):
        for d in range(1, n_sp):
            for u in range(3 * g, 3 * g + 3):
                copy = remote(
                    piece(u, (z + d) % n_sp),
                    w_all.at[block(z), pl.ds(u * wide, wide)],
                    z_send.at[d, u],
                    z_recv.at[d, u],
                    sp=(z + d) % n_sp,
                )
                copy.start()
                z_copies[d, u] = copy

    def part(owner_z, owner_f, g):
        start = pl.multiple_of((owner_z * fs + owner_f) * rows, rows)
        return w_all.at[pl.ds(start, rows), pl.ds(g * group, group)]

    x_copies, y_copies = {}, {}
    for d in range(n_sp):
        owner = (z + n_sp - d) % n_sp
        for g in range(2):
            for u in range(3 * g, 3 * g + 3):
                if d == 0:
                    locals_[u].wait()
                else:
                    z_copies[d, u].wait_recv()
            ref = part(owner, f, g)
            x_copies[d, g] = remote(ref, ref, x_send.at[d, g], x_recv.at[d, g], fs=xn)
            y_copies[d, g] = remote(ref, ref, y_send.at[d, g], y_recv.at[d, g], fs=yn)
            x_copies[d, g].start()
            y_copies[d, g].start()

    for d in range(1, n_sp):
        owner = (z + n_sp - d) % n_sp
        tok_copies[d].wait_recv()
        ref = tok_all.at[owner, mine]
        copy = remote(ref, ref, p_send.at[d], p_recv.at[d], tp=other)
        copy.start()
        pending.append(copy)

    for d in range(n_sp):
        owner = (z + n_sp - d) % n_sp
        x_copies[d, 0].wait_recv()
        ref = part(owner, xn, 0)
        copy = remote(ref, ref, yf_send.at[d], yf_recv.at[d], fs=yn)
        copy.start()
        pending.append(copy)
        y_copies[d, 1].wait_recv()
        ref = part(owner, yn, 1)
        copy = remote(ref, ref, xf_send.at[d], xf_recv.at[d], fs=xn)
        copy.start()
        pending.append(copy)

    for d in range(n_sp):
        x_copies[d, 1].wait_recv()
        y_copies[d, 0].wait_recv()
    for copy in pending:
        copy.wait()
    for d in range(1, n_sp):
        tok_copies[d].wait_send()
    for copy in list(z_copies.values()) + list(x_copies.values()) + list(y_copies.values()):
        copy.wait_send()
    own_tok.wait()
    own_shift.wait()


def gather_all(n_sp, tokens, lat, wq, wk, wv, wr, wa, shift):
    rows, width = tokens.shape
    dma = pltpu.SemaphoreType.DMA
    return pl.pallas_call(
        functools.partial(gather_kernel, n_sp),
        out_shape=(
            jax.ShapeDtypeStruct((n_sp, rows, width), tokens.dtype),
            jax.ShapeDtypeStruct((n_sp * 4 * rows, 6 * lat.shape[2]), lat.dtype),
            jax.ShapeDtypeStruct((n_sp,) + shift.shape, shift.dtype),
        ),
        in_specs=[pl.BlockSpec(memory_space=pl.ANY)] * 8,
        out_specs=(pl.BlockSpec(memory_space=pl.ANY),) * 3,
        scratch_shapes=[
            dma((8,)),
            dma((n_sp, 6)),
            dma((n_sp, 6)),
            dma((n_sp, 2)),
            dma((n_sp, 2)),
            dma((n_sp, 2)),
            dma((n_sp, 2)),
            dma((n_sp,)),
            dma((n_sp,)),
            dma((n_sp,)),
            dma((n_sp,)),
            dma((n_sp,)),
            dma((n_sp,)),
            dma((n_sp,)),
            dma((n_sp,)),
            dma((n_sp,)),
            dma((n_sp,)),
        ],
        compiler_params=pltpu.CompilerParams(collective_id=0, has_side_effects=True),
    )(tokens, lat, wq, wk, wv, wr, wa, shift)


def heads_plan(
    tokens,
    norm_gain,
    w_ret_query,
    w_ret_key,
    w_ret_value,
    w_q_down,
    w_kv_down,
    w_rope_key,
    w_q_up,
    w_kv_up,
    q_lat_gain,
    kv_lat_gain,
    att_norm_gain,
    ret_norm_gain,
    w_ret_out,
    w_att_out,
    head_rate,
    decay_shift,
    start_state,
):
    n_sp, n_tp = lax.axis_size("sp"), lax.axis_size("tp")
    z = lax.axis_index("sp")
    rows = tokens.shape[1]
    length = n_sp * rows
    q_part = w_q_down.shape[1] // n_sp
    kv_part = w_kv_down.shape[1] // n_sp
    rope_half = ROPE_DIM // 2
    rope_part = rope_half // n_sp
    att_heads = w_q_up.shape[1] // (NOPE_DIM + ROPE_DIM) // n_sp
    w_rows = w_q_down.shape[0]
    lat = jnp.concatenate(
        [
            w_q_down.reshape(w_rows, n_sp, q_part),
            w_kv_down.reshape(w_rows, n_sp, kv_part),
            w_rope_key.reshape(w_rows, 2, n_sp, rope_part)
            .transpose(0, 2, 1, 3)
            .reshape(w_rows, n_sp, 2 * rope_part),
        ],
        axis=2,
    ).transpose(1, 0, 2)
    lat = jnp.pad(lat, ((0, 0), (0, 0), (0, RET_DIM - lat.shape[2])))
    tok_all, w_all, shift_all = gather_all(
        n_sp,
        tokens[0],
        lat,
        w_ret_query,
        w_ret_key,
        w_ret_value,
        w_ret_out,
        w_att_out,
        decay_shift[0],
    )
    positions = jnp.arange(length, dtype=jnp.int32)
    ret_cos, ret_sin = angle_tables(positions, RET_DIM)
    rope_cos, rope_sin = angle_tables(positions, ROPE_DIM)
    source = tok_all.reshape(length, -1).astype(jnp.float32)
    normed = rms_scale(source, norm_gain).astype(jnp.bfloat16)
    projected = jnp.dot(normed, w_all[:, : 4 * RET_DIM], preferred_element_type=jnp.float32)
    rope_at = q_part + kv_part
    cos_part = lax.dynamic_slice_in_dim(rope_cos, z * rope_part, rope_part, 1)
    sin_part = lax.dynamic_slice_in_dim(rope_sin, z * rope_part, rope_part, 1)
    sent = jnp.concatenate(
        [
            projected[:, :rope_at],
            rotate(projected[:, rope_at : rope_at + 2 * rope_part], cos_part, sin_part),
        ],
        axis=1,
    ).astype(jnp.bfloat16)
    lats = lax.all_gather(sent, ("tp", "sp"), axis=0)
    lat_q_raw = lats[:, :, :q_part].transpose(1, 0, 2).reshape(length, -1)
    lat_kv_raw = lats[:, :, q_part:rope_at].transpose(1, 0, 2).reshape(length, -1)
    rope_key = (
        lats[:n_sp, :, rope_at:]
        .reshape(n_sp, length, 2, rope_part)
        .transpose(1, 2, 0, 3)
        .reshape(length, ROPE_DIM)
    )

    ret_q = rotate(projected[:, RET_DIM : 2 * RET_DIM], ret_cos, ret_sin).astype(jnp.bfloat16)
    ret_k = (
        rotate(projected[:, 2 * RET_DIM : 3 * RET_DIM], ret_cos, ret_sin) * RET_DIM ** (-0.5)
    ).astype(jnp.bfloat16)
    ret_v = projected[:, 3 * RET_DIM : 4 * RET_DIM].astype(jnp.bfloat16)
    rate = lax.dynamic_index_in_dim(head_rate, z, 0, keepdims=False)
    shift = lax.dynamic_index_in_dim(shift_all, z, 1, keepdims=False)
    cumul = jnp.cumsum(rate + shift, axis=1)
    last = cumul[:, -1]
    offsets = jnp.arange(rows, dtype=jnp.int32)
    lower = offsets[None, :] <= offsets[:, None]
    decay = jnp.exp(jnp.where(lower[None], cumul[:, :, None] - cumul[:, None, :], -jnp.inf))
    bq, bk, bv = (a.reshape(n_sp, rows, RET_DIM) for a in (ret_q, ret_k, ret_v))
    scores = (
        jnp.einsum("bnd,bmd->bnm", bq, bk, preferred_element_type=jnp.float32) * decay
    ).astype(jnp.bfloat16)
    inside = jnp.einsum("bnm,bme->bne", scores, bv, preferred_element_type=jnp.float32)
    weighted = bk.astype(jnp.float32) * jnp.exp(last[:, None] - cumul)[:, :, None]
    added = jnp.einsum(
        "bmd,bme->bde", weighted, bv.astype(jnp.float32), precision=TOP_PRECISION
    )
    state = lax.dynamic_index_in_dim(start_state[0], z, 0, keepdims=False)
    states = []
    for b in range(n_sp):
        states.append(state)
        state = jnp.exp(last[b]) * state + added[b]
    carried = (
        jnp.einsum(
            "bnd,bde->bne", bq.astype(jnp.float32), jnp.stack(states), precision=TOP_PRECISION
        )
        * jnp.exp(cumul)[:, :, None]
    )
    ret_raw = (inside + carried).reshape(length, RET_DIM)
    row_mean = jnp.mean(ret_raw, axis=-1, keepdims=True)
    centered = ret_raw - row_mean
    row_var = jnp.mean(centered * centered, axis=-1, keepdims=True)
    ret_gain = lax.dynamic_slice_in_dim(ret_norm_gain, z * RET_DIM, RET_DIM, 0)
    ret_out = (centered * lax.rsqrt(row_var + EPSILON) * ret_gain).astype(jnp.bfloat16)

    q_latent = rms_scale(lat_q_raw.astype(jnp.float32), q_lat_gain).astype(jnp.bfloat16)
    kv_latent = rms_scale(lat_kv_raw.astype(jnp.float32), kv_lat_gain).astype(jnp.bfloat16)
    q_wide = att_heads * (NOPE_DIM + ROPE_DIM)
    kv_wide = att_heads * (NOPE_DIM + VAL_DIM)
    q_up = lax.dynamic_slice_in_dim(w_q_up, z * q_wide, q_wide, 1)
    kv_up = lax.dynamic_slice_in_dim(w_kv_up, z * kv_wide, kv_wide, 1)
    query = jnp.dot(q_latent, q_up, preferred_element_type=jnp.float32)
    expanded = jnp.dot(kv_latent, kv_up, preferred_element_type=jnp.float32).astype(jnp.bfloat16)
    att_gain = lax.dynamic_slice_in_dim(
        att_norm_gain, z * att_heads * VAL_DIM, att_heads * VAL_DIM, 0
    )
    allowed = positions[None, :] <= positions[:, None]
    outs = [ret_out]
    for h in range(att_heads):
        q_h = query[:, h * (NOPE_DIM + ROPE_DIM) : (h + 1) * (NOPE_DIM + ROPE_DIM)]
        q_h = jnp.concatenate(
            [q_h[:, :NOPE_DIM], rotate(q_h[:, NOPE_DIM:], rope_cos, rope_sin)], axis=1
        ).astype(jnp.bfloat16)
        kv_h = expanded[:, h * (NOPE_DIM + VAL_DIM) : (h + 1) * (NOPE_DIM + VAL_DIM)]
        k_h = jnp.concatenate([kv_h[:, :NOPE_DIM], rope_key], axis=1)
        s = lax.dot_general(
            q_h, k_h, (((1,), (1,)), ((), ())), preferred_element_type=jnp.float32
        ) * (NOPE_DIM + ROPE_DIM) ** (-0.5)
        s = jnp.where(allowed, s, -jnp.inf)
        p = jnp.exp(s - jnp.max(s, axis=-1, keepdims=True))
        total = jnp.sum(p, axis=-1, keepdims=True)
        raw = (
            jnp.dot(
                p.astype(jnp.bfloat16), kv_h[:, NOPE_DIM:], preferred_element_type=jnp.float32
            )
            / total
        )
        outs.append(
            rms_scale(raw, att_gain[h * VAL_DIM : (h + 1) * VAL_DIM]).astype(jnp.bfloat16)
        )
    merged = jnp.concatenate(outs, axis=1)
    partial_sum = lax.dot_general(
        merged,
        w_all[:, 4 * RET_DIM :],
        (((1,), (1,)), ((), ())),
        preferred_element_type=jnp.float32,
    ).astype(jnp.bfloat16)
    mixed = lax.psum_scatter(partial_sum, ("sp", "tp"), scatter_dimension=0, tiled=True)
    return mixed[None]


def solution(mesh):
    placed = (
        P("fs", "sp", None),
        P(),
        P(("sp", "fs"), "tp"),
        P(("sp", "fs"), "tp"),
        P(("sp", "fs"), "tp"),
        P(("sp", "fs"), "tp"),
        P(("sp", "fs"), "tp"),
        P(("sp", "fs"), None),
        P(None, "tp"),
        P(None, "tp"),
        P(),
        P(),
        P("tp"),
        P("tp"),
        P(("sp", "fs"), "tp"),
        P(("sp", "fs"), "tp"),
        P("tp"),
        P("fs", "tp", "sp"),
        P("fs", "tp", None, None),
    )

    def pick(*args):
        if heads_fit(mesh, args[16].shape[0], args[0].shape[0]):
            return heads_plan(*args)
        return rows_plan(*args)

    return jax.shard_map(
        pick,
        mesh=mesh,
        in_specs=placed,
        out_specs=P("fs", ("sp", "tp"), None),
        check_vma=False,
    )
```

```python
import functools

import jax
import jax.numpy as jnp
from jax import lax
from jax.experimental import pallas as pl
from jax.experimental.pallas import tpu as pltpu
from jax.sharding import PartitionSpec as P

RET_DIM = 256
NOPE_DIM = 128
ROPE_DIM = 64
VAL_DIM = 128
KV_LAT = 512


EPSILON = 1e-06
THETA_BASE = 10000.0
TOP_PRECISION = lax.Precision.HIGHEST


def prefix(x, axis, combine, identity):
    peers, position = (lax.axis_size(axis), lax.axis_index(axis))
    everything = jax.tree.map(
        lambda part, kind: lax.all_gather(part.astype(kind), axis), x, (jnp.bfloat16, jnp.bfloat16)
    )
    start = jax.tree.map(
        lambda part, zero: jnp.broadcast_to(jnp.asarray(zero, part.dtype), part.shape), x, identity
    )

    def lap(k, before):
        reached = k < position
        new = combine(
            before, jax.tree.map(lambda part, own: part[k].astype(own.dtype), everything, x)
        )
        return jax.tree.map(lambda a, b: jnp.where(reached, a, b), new, before)

    return lax.fori_loop(0, peers, lap, start)


def angle_tables(positions, rot_width):
    half_width = rot_width // 2
    inverse = THETA_BASE ** (-jnp.arange(half_width, dtype=jnp.float32) * 2.0 / rot_width)
    angles = positions.astype(jnp.float32)[:, None] * inverse[None, :]
    return (jnp.cos(angles), jnp.sin(angles))


def rotate(values, cosine, sine):
    half_width = values.shape[-1] // 2
    front_half = values[..., :half_width]
    back_half = values[..., half_width:]
    return jnp.concatenate(
        [front_half * cosine - back_half * sine, back_half * cosine + front_half * sine], axis=-1
    )


def rms_scale(values, gain_vector):
    return (
        values
        * lax.rsqrt(jnp.mean(values * values, axis=-1, keepdims=True) + EPSILON)
        * gain_vector
    )


def chain_states(earlier, later):
    early_log, early_state = earlier
    late_log, late_state = later
    return (early_log + late_log, jnp.exp(late_log)[:, None, None] * early_state + late_state)


def rows_plan(
    tokens,
    norm_gain,
    w_ret_query,
    w_ret_key,
    w_ret_value,
    w_q_down,
    w_kv_down,
    w_rope_key,
    w_q_up,
    w_kv_up,
    q_lat_gain,
    kv_lat_gain,
    att_norm_gain,
    ret_norm_gain,
    w_ret_out,
    w_att_out,
    head_rate,
    decay_shift,
    start_state,
):
    tok_rows = tokens.shape[1]
    ret_local = head_rate.shape[0]
    att_local = w_q_up.shape[1] // (NOPE_DIM + ROPE_DIM)
    row_offset = lax.axis_index("sp") * tok_rows
    positions = row_offset + jnp.arange(tok_rows, dtype=jnp.int32)
    (
        full_query,
        full_key,
        full_value,
        full_q_down,
        full_kv_down,
        full_rope,
        full_ret_out,
        full_att_out,
    ) = (
        lax.all_gather(w_ret_query, ("sp", "fs"), axis=0, tiled=True),
        lax.all_gather(w_ret_key, ("sp", "fs"), axis=0, tiled=True),
        lax.all_gather(w_ret_value, ("sp", "fs"), axis=0, tiled=True),
        lax.all_gather(w_q_down, ("sp", "fs"), axis=0, tiled=True),
        lax.all_gather(w_kv_down, ("sp", "fs"), axis=0, tiled=True),
        lax.all_gather(w_rope_key, ("sp", "fs"), axis=0, tiled=True),
        lax.all_gather(w_ret_out, ("sp", "fs"), axis=0, tiled=True),
        lax.all_gather(w_att_out, ("sp", "fs"), axis=0, tiled=True),
    )
    source = tokens[0].astype(jnp.float32)
    normed = rms_scale(source, norm_gain).astype(jnp.bfloat16)
    ret_cos, ret_sin = angle_tables(positions, RET_DIM)
    rope_cos, rope_sin = angle_tables(positions, ROPE_DIM)

    def project(weight):
        return jnp.dot(normed, weight, preferred_element_type=jnp.float32)

    part_q = project(full_q_down).astype(jnp.bfloat16)
    part_kv = project(full_kv_down).astype(jnp.bfloat16)
    lat_q_raw, lat_kv_raw = (
        lax.all_gather(part_q, "tp", axis=1, tiled=True),
        lax.all_gather(part_kv, "tp", axis=1, tiled=True),
    )
    retention_query = rotate(
        project(full_query).reshape(tok_rows, ret_local, RET_DIM),
        ret_cos[:, None],
        ret_sin[:, None],
    ).astype(jnp.bfloat16)
    retention_key = (
        rotate(
            project(full_key).reshape(tok_rows, ret_local, RET_DIM),
            ret_cos[:, None],
            ret_sin[:, None],
        )
        * RET_DIM ** (-0.5)
    ).astype(jnp.bfloat16)
    retention_value = project(full_value).reshape(tok_rows, ret_local, RET_DIM).astype(jnp.bfloat16)
    rope_key = rotate(project(full_rope), rope_cos, rope_sin).astype(jnp.bfloat16)
    log_rates = head_rate[:, None] + decay_shift[0]
    cumul = jnp.cumsum(log_rates, axis=1)
    offsets = jnp.arange(tok_rows, dtype=jnp.int32)
    lower_mask = offsets[None, :] <= offsets[:, None]
    decay_matrix = jnp.exp(
        jnp.where(lower_mask[None], cumul[:, :, None] - cumul[:, None, :], -jnp.inf)
    )
    block_score_grid = (
        jnp.einsum(
            "zgq,ugq->gzu", retention_query, retention_key, preferred_element_type=jnp.float32
        )
        * decay_matrix
    ).astype(jnp.bfloat16)
    inside_block_output = jnp.einsum(
        "vzs,svp->zvp", block_score_grid, retention_value, preferred_element_type=jnp.float32
    )
    block_output_sum = cumul[:, -1]
    weighted_values = (
        retention_key.astype(jnp.float32) * jnp.exp(block_output_sum[:, None] - cumul).T[:, :, None]
    )
    contribution = jnp.einsum(
        "uzj,uzv->zjv",
        weighted_values,
        retention_value.astype(jnp.float32),
        precision=TOP_PRECISION,
    )
    identity = (jnp.zeros_like(block_output_sum), jnp.zeros_like(contribution))
    before_log, before_state = prefix(
        (block_output_sum, contribution), "sp", chain_states, identity
    )
    q_latent = rms_scale(lat_q_raw.astype(jnp.float32), q_lat_gain).astype(jnp.bfloat16)
    kv_latent = rms_scale(lat_kv_raw.astype(jnp.float32), kv_lat_gain).astype(jnp.bfloat16)
    query_full = jnp.dot(q_latent, w_q_up, preferred_element_type=jnp.float32).reshape(
        tok_rows, att_local, NOPE_DIM + ROPE_DIM
    )
    query_nope = query_full[..., :NOPE_DIM].astype(jnp.bfloat16)
    query_rope = rotate(query_full[..., NOPE_DIM:], rope_cos[:, None], rope_sin[:, None]).astype(
        jnp.bfloat16
    )
    att_scale = (NOPE_DIM + ROPE_DIM) ** (-0.5)

    def attend(carry, key_nope, key_values, key_rope, start):
        running_max, running_sum, running_acc = carry
        key_count = key_rope.shape[0]
        score_matrix = (
            jnp.einsum("qhd,khd->hqk", query_nope, key_nope, preferred_element_type=jnp.float32)
            + jnp.einsum("qhd,kd->hqk", query_rope, key_rope, preferred_element_type=jnp.float32)
        ) * att_scale
        key_positions = start + jnp.arange(key_count, dtype=jnp.int32)
        allowed = key_positions[None, :] <= positions[:, None]
        masked = jnp.where(allowed[None], score_matrix, -jnp.inf)
        new_max = jnp.maximum(running_max, jnp.max(masked, axis=-1))
        safe_max = jnp.where(jnp.isfinite(new_max), new_max, 0.0)
        weights = jnp.exp(masked - safe_max[..., None])
        rescale = jnp.exp(running_max - safe_max)
        new_sum = running_sum * rescale + jnp.sum(weights, axis=-1)
        new_acc = running_acc * rescale[..., None] + jnp.einsum(
            "hqk,khd->hqd",
            weights.astype(jnp.bfloat16),
            key_values,
            preferred_element_type=jnp.float32,
        )
        return (new_max, new_sum, new_acc)

    def expand_attend(carry_in, lat_piece, rope_piece, start):
        wide = (
            jnp.dot(lat_piece, w_kv_up, preferred_element_type=jnp.float32)
            .astype(jnp.bfloat16)
            .reshape(rope_piece.shape[0], att_local, NOPE_DIM + VAL_DIM)
        )
        return attend(carry_in, wide[..., :NOPE_DIM], wide[..., NOPE_DIM:], rope_piece, start)

    empty = (
        jnp.full((att_local, tok_rows), -jnp.inf, jnp.float32),
        jnp.zeros((att_local, tok_rows), jnp.float32),
        jnp.zeros((att_local, tok_rows, VAL_DIM), jnp.float32),
    )
    groups = lax.axis_size("tp")
    kv_part = KV_LAT // groups
    rope_part = ROPE_DIM // groups
    my_group = lax.axis_index("tp")
    joined = jnp.concatenate(
        [
            lax.dynamic_slice_in_dim(kv_latent, my_group * kv_part, kv_part, 1),
            lax.dynamic_slice_in_dim(rope_key, my_group * rope_part, rope_part, 1),
        ],
        axis=1,
    )
    all_rows = lax.all_gather(joined, "sp", axis=0, tiled=True)
    complete = lax.all_gather(all_rows, "tp", axis=1, tiled=True)
    total_rows = complete.shape[0]
    grouped = complete.reshape(total_rows, groups, kv_part + rope_part)
    lat_all = grouped[:, :, :kv_part].reshape(total_rows, KV_LAT)
    rope_all = grouped[:, :, kv_part:].reshape(total_rows, ROPE_DIM)

    def visit(block_index, carry_in):
        start = block_index * tok_rows
        lat_piece = lax.dynamic_slice_in_dim(lat_all, start, tok_rows, 0)
        rope_piece = lax.dynamic_slice_in_dim(rope_all, start, tok_rows, 0)
        return expand_attend(carry_in, lat_piece, rope_piece, start)

    final = lax.fori_loop(0, lax.axis_index("sp") + 1, visit, empty)
    att_raw = jnp.transpose(final[2] / final[1][..., None], (1, 0, 2))
    att_out = (
        rms_scale(att_raw, att_norm_gain.reshape(att_local, VAL_DIM))
        .astype(jnp.bfloat16)
        .reshape(tok_rows, att_local * VAL_DIM)
    )
    entering = jnp.exp(before_log)[:, None, None] * start_state[0] + before_state
    carried_term = (
        jnp.einsum(
            "nhd,hde->nhe", retention_query.astype(jnp.float32), entering, precision=TOP_PRECISION
        )
        * jnp.exp(cumul).T[:, :, None]
    )
    ret_raw = inside_block_output + carried_term
    row_mean = jnp.mean(ret_raw, axis=-1, keepdims=True)
    centered = ret_raw - row_mean
    row_var = jnp.mean(centered * centered, axis=-1, keepdims=True)
    ret_out = (
        (centered * lax.rsqrt(row_var + EPSILON) * ret_norm_gain.reshape(ret_local, RET_DIM))
        .astype(jnp.bfloat16)
        .reshape(tok_rows, ret_local * RET_DIM)
    )
    contract = (((1,), (1,)), ((), ()))
    mixed = lax.psum_scatter(
        (
            lax.dot_general(ret_out, full_ret_out, contract, preferred_element_type=jnp.float32)
            + lax.dot_general(att_out, full_att_out, contract, preferred_element_type=jnp.float32)
        ).astype(jnp.bfloat16),
        "tp",
        scatter_dimension=0,
        tiled=True,
    )
    return mixed[None]


MESH = pl.DeviceIdType.MESH
WIDE = RET_DIM
CONTRACT = (((1,), (1,)), ((), ()))
GROUPS = ((0, 2), (2, 2), (4, 1), (5, 1))
FIRST, LATER = (0, 1), (2, 3)


def heads_fit(mesh, ret_local, sequences, q_wide, kv_wide):
    sizes = mesh.shape
    return (
        sizes["fs"] == 4
        and sizes["tp"] == 2
        and ret_local == sizes["sp"]
        and sequences == 1
        and q_wide % 128 == 0
        and kv_wide % 128 == 0
        and q_wide + kv_wide + 2 * ROPE_DIM <= ret_local * WIDE
    )


def three_parts(x):
    high = x.astype(jnp.bfloat16)
    rest = x - high.astype(jnp.float32)
    middle = rest.astype(jnp.bfloat16)
    low = (rest - middle.astype(jnp.float32)).astype(jnp.bfloat16)
    return high, middle, low


def layer_kernel(
    n_sp,
    q_wide,
    kv_wide,
    tok_ref,
    lat_ref,
    wq_ref,
    wk_ref,
    wv_ref,
    wr_ref,
    wa_ref,
    shift_ref,
    rate_ref,
    gain_ref,
    qgain_ref,
    kvgain_ref,
    again_ref,
    rgain_ref,
    rcos_ref,
    rsin_ref,
    pcos_ref,
    psin_ref,
    qup_ref,
    kvup_ref,
    start_ref,
    out_ref,
    tok_all,
    w_all,
    shift_all,
    normed,
    acc,
    ret_q,
    ret_k,
    ret_v,
    lat_all,
    state,
    qn,
    qr,
    expanded,
    rope_key,
    kvup,
    merged,
    own_sum,
    pair_out,
    pair_in,
    row_out,
    row_in,
    local_sem,
    z_send,
    z_recv,
    x_send,
    x_recv,
    y_send,
    y_recv,
    f_send,
    f_recv,
    m_send,
    m_recv,
):
    z, f, t = lax.axis_index("sp"), lax.axis_index("fs"), lax.axis_index("tp")
    xn = f + 1 - 2 * (f % 2)
    yn = (f + 2) % 4
    other = 1 - t
    fs = 4
    rows = tok_ref.shape[0]
    half = rows // 2
    weights = (lat_ref, wq_ref, wk_ref, wv_ref, wr_ref, wa_ref)
    f32, bf16 = jnp.float32, jnp.bfloat16

    def remote(src, dst, send, recv, **where):
        return pltpu.make_async_remote_copy(
            src_ref=src,
            dst_ref=dst,
            send_sem=send,
            recv_sem=recv,
            device_id={"sp": z, "fs": f, "tp": t, **where},
            device_id_type=MESH,
        )

    barrier = pltpu.get_barrier_semaphore()
    peers = [{"sp": (z + d) % n_sp, "fs": f, "tp": t} for d in range(1, n_sp)]
    peers += [{"sp": z, "fs": xn, "tp": t}, {"sp": z, "fs": yn, "tp": t}]
    peers += [{"sp": z, "fs": f, "tp": other}]
    for peer in peers:
        pl.semaphore_signal(barrier, inc=1, device_id=peer, device_id_type=MESH)
    pl.semaphore_wait(barrier, len(peers))

    def piece(u, owner):
        return weights[u].at[:, pl.ds(pl.multiple_of(owner * WIDE, WIDE), WIDE)]

    def part(owner_z, owner_f, g):
        first, count = GROUPS[g]
        start = pl.multiple_of((owner_z * fs + owner_f) * rows, rows)
        return w_all.at[pl.ds(start, rows), pl.ds(first * WIDE, count * WIDE)]

    def unit(u):
        start = pl.multiple_of((z * fs + f) * rows, rows)
        return w_all.at[pl.ds(start, rows), pl.ds(u * WIDE, WIDE)]

    pending = []

    def go(copy):
        copy.start()
        pending.append(copy)
        return copy

    def owner(d):
        return (z + n_sp - d) % n_sp

    mine = pl.ds(pl.multiple_of(t * half, half), half)
    tok_copies, z_copies, x_copies, y_copies, f_copies = {}, {}, {}, {}, {}
    for d in range(1, n_sp):
        to = (z + d) % n_sp
        tok_copies[d] = remote(
            tok_ref.at[mine], tok_all.at[z, mine], m_send.at[0, d], m_recv.at[0, d], sp=to
        )
        tok_copies[d].start()
    for d in range(1, n_sp):
        to = (z + d) % n_sp
        go(remote(shift_ref, shift_all.at[z], m_send.at[2, d], m_recv.at[2, d], sp=to))
    shift_copies = list(pending)
    pending.clear()
    locals_ = []
    for u in range(6):
        copy = pltpu.make_async_copy(piece(u, z), unit(u), local_sem.at[u])
        copy.start()
        locals_.append(copy)
    own_tok = pltpu.make_async_copy(tok_ref, tok_all.at[z], local_sem.at[6])
    own_tok.start()
    own_shift = pltpu.make_async_copy(shift_ref, shift_all.at[z], local_sem.at[7])
    own_shift.start()
    att_wide = kvup.shape[1]
    own_kvup = pltpu.make_async_copy(
        kvup_ref.at[:, pl.ds(pl.multiple_of(z * att_wide, att_wide), att_wide)],
        kvup,
        local_sem.at[8],
    )
    own_kvup.start()
    own_state = pltpu.make_async_copy(start_ref.at[z], state, local_sem.at[9])
    own_state.start()
    for group in (FIRST, LATER):
        for d in range(1, n_sp):
            to = (z + d) % n_sp
            for g in group:
                for u in range(GROUPS[g][0], sum(GROUPS[g])):
                    z_copies[d, u] = remote(
                        piece(u, to), unit(u), z_send.at[d, u], z_recv.at[d, u], sp=to
                    )
                    z_copies[d, u].start()

    def spread(d, group):
        for g in group:
            for u in range(GROUPS[g][0], sum(GROUPS[g])):
                if d == 0:
                    locals_[u].wait()
                else:
                    z_copies[d, u].wait_recv()
            ref = part(owner(d), f, g)
            x_copies[d, g] = remote(ref, ref, x_send.at[d, g], x_recv.at[d, g], fs=xn)
            y_copies[d, g] = remote(ref, ref, y_send.at[d, g], y_recv.at[d, g], fs=yn)
            x_copies[d, g].start()
            y_copies[d, g].start()

    def relay(d, group):
        for g in group:
            if g % 2 == 0:
                x_copies[d, g].wait_recv()
                ref, to = part(owner(d), xn, g), yn
            else:
                y_copies[d, g].wait_recv()
                ref, to = part(owner(d), yn, g), xn
            f_copies[d, g] = remote(ref, ref, f_send.at[d, g], f_recv.at[d, g], fs=to)
            f_copies[d, g].start()

    def arrive(d, group):
        for g in group:
            if g % 2 == 0:
                y_copies[d, g].wait_recv()
            else:
                x_copies[d, g].wait_recv()
            f_copies[d, g].wait_recv()

    def at(i):
        return pl.ds(pl.multiple_of(i * rows, rows), rows)

    def norm_block(i):
        x = tok_all[i].astype(f32)
        scaled = x * lax.rsqrt(jnp.mean(x * x, axis=-1, keepdims=True) + EPSILON)
        normed[at(i), :] = (scaled * gain_ref[...]).astype(bf16)

    spread(0, FIRST)
    own_tok.wait()
    norm_block(z)
    tok_pair = {}
    for d in range(1, n_sp):
        tok_copies[d].wait_recv()
        ref = tok_all.at[owner(d), mine]
        tok_pair[d] = go(remote(ref, ref, m_send.at[1, d], m_recv.at[1, d], tp=other))
    for d in range(1, n_sp):
        spread(d, FIRST)
        relay(d - 1, FIRST)
        tok_pair[d].wait_recv()
        norm_block(owner(d))
    relay(n_sp - 1, FIRST)
    spread(0, LATER)
    depth = fs * rows
    for d in range(n_sp):
        arrive(d, FIRST)
        begin = pl.multiple_of(owner(d) * depth, depth)

        def multiply(i, carry, d=d, begin=begin):
            got = jnp.dot(
                normed[at(i), pl.ds(begin, depth)],
                w_all[pl.ds(begin, depth), : 4 * WIDE],
                preferred_element_type=f32,
            )
            if d == 0:
                acc[at(i), :] = got
            else:
                acc[at(i), :] += got
            return carry

        lax.fori_loop(0, n_sp, multiply, 0)

    rope_index = (q_wide + kv_wide) // WIDE
    rope_lane = (q_wide + kv_wide) % WIDE
    rd = RET_DIM // 2

    def finish_lat(i, carry):
        raw = acc[at(i), :WIDE]
        pair = raw[:, rope_lane : rope_lane + 2 * ROPE_DIM]
        turned = pair * pcos_ref[at(i), :] + pltpu.roll(pair, ROPE_DIM, 1) * psin_ref[at(i), :]
        lane = lax.broadcasted_iota(jnp.int32, turned.shape, 1)
        turned = jnp.where(lane < ROPE_DIM, turned, pltpu.roll(turned, ROPE_DIM, 1))
        pieces = [raw[:, :rope_lane]] if rope_lane else []
        pieces.append(jnp.where(z == rope_index, turned, pair))
        if rope_lane + 2 * ROPE_DIM < WIDE:
            pieces.append(raw[:, rope_lane + 2 * ROPE_DIM :])
        lat_all[t, z, at(i), :] = jnp.concatenate(pieces, axis=1).astype(bf16)
        return carry

    lax.fori_loop(0, n_sp, finish_lat, 0)
    lat_copies = {}
    lat_own = lat_all.at[t, z]
    lat_pair = {0: go(remote(lat_own, lat_own, m_send.at[4, 0], m_recv.at[4, 0], tp=other))}
    for d in range(1, n_sp):
        lat_copies[d] = remote(
            lat_own, lat_own, m_send.at[3, d], m_recv.at[3, d], sp=(z + d) % n_sp
        )
        lat_copies[d].start()

    def finish_ret(i, carry):
        cosine, sine = rcos_ref[at(i), :], rsin_ref[at(i), :]
        for dst, base, factor in ((ret_q, WIDE, 1.0), (ret_k, 2 * WIDE, RET_DIM ** (-0.5))):
            a, b = acc[at(i), base : base + rd], acc[at(i), base + rd : base + WIDE]
            dst[at(i), :rd] = ((a * cosine - b * sine) * factor).astype(bf16)
            dst[at(i), rd:] = ((b * cosine + a * sine) * factor).astype(bf16)
        ret_v[at(i), :] = acc[at(i), 3 * WIDE :].astype(bf16)
        return carry

    lax.fori_loop(0, n_sp, finish_ret, 0)

    for copy in shift_copies:
        copy.wait()
    own_shift.wait()
    own_state.wait()
    r_iota = lax.broadcasted_iota(jnp.int32, (rows, rows), 0)
    c_iota = lax.broadcasted_iota(jnp.int32, (rows, rows), 1)

    def retention(b):
        rates = shift_all[b] + rate_ref[...]
        pick = lax.broadcasted_iota(jnp.int32, rates.shape, 0) == z
        row = jnp.sum(jnp.where(pick, rates, 0.0), axis=0, keepdims=True)
        column = jnp.sum(jnp.where(r_iota == c_iota, row, 0.0), axis=1, keepdims=True)
        c_col = jnp.sum(jnp.where(c_iota <= r_iota, row, 0.0), axis=1, keepdims=True)
        c_row = jnp.sum(jnp.where(r_iota <= c_iota, column, 0.0), axis=0, keepdims=True)
        last = jnp.sum(row, axis=1, keepdims=True)
        decay = jnp.exp(jnp.where(c_iota <= r_iota, c_col - c_row, -jnp.inf))
        block = slice(b * rows, (b + 1) * rows)
        q, k, v = ret_q[block, :], ret_k[block, :], ret_v[block, :]
        scores = lax.dot_general(q, k, CONTRACT, preferred_element_type=f32) * decay
        raw = jnp.dot(scores.astype(bf16), v, preferred_element_type=f32)
        carried = sum(
            jnp.dot(q, s, preferred_element_type=f32) for s in three_parts(state[...])
        )
        raw = raw + carried * jnp.exp(c_col)
        if b < n_sp - 1:
            weighted = k.astype(f32) * jnp.exp(last - c_col)
            added = sum(
                lax.dot_general(w, v, (((0,), (0,)), ((), ())), preferred_element_type=f32)
                for w in three_parts(weighted)
            )
            state[...] = jnp.exp(last) * state[...] + added
        centered = raw - jnp.mean(raw, axis=-1, keepdims=True)
        variance = jnp.mean(centered * centered, axis=-1, keepdims=True)
        merged[block, :WIDE] = (centered * lax.rsqrt(variance + EPSILON) * rgain_ref[z]).astype(
            bf16
        )

    for b in range(n_sp):
        if b:
            spread(b, LATER)
            relay(b - 1, LATER)
            lat_copies[b].wait_recv()
            ref = lat_all.at[t, owner(b)]
            lat_pair[b] = go(remote(ref, ref, m_send.at[4, b], m_recv.at[4, b], tp=other))
        retention(b)
    relay(n_sp - 1, LATER)
    for d in range(n_sp):
        lat_pair[d].wait_recv()
    own_kvup.wait()

    def chunks(first, count):
        found = []
        for core in range(2):
            for j in range(count // 128):
                lane = first + j * 128
                found.append((core, lane // WIDE, lane % WIDE))
        return found

    q_chunks, kv_chunks = chunks(0, q_wide), chunks(q_wide, kv_wide)
    rope_at = (rope_index, rope_lane)
    att_heads = att_wide // (NOPE_DIM + VAL_DIM)
    nope = att_heads * NOPE_DIM
    turn = att_heads * ROPE_DIM

    def expand(i, carry):
        def latent(found, gain):
            x = jnp.concatenate(
                [lat_all[c, s, at(i), lane : lane + 128] for c, s, lane in found], axis=1
            ).astype(f32)
            scaled = x * lax.rsqrt(jnp.mean(x * x, axis=-1, keepdims=True) + EPSILON)
            return (scaled * gain[...]).astype(bf16)

        query = jnp.dot(latent(q_chunks, qgain_ref), qup_ref[...], preferred_element_type=f32)
        qn[at(i), :] = query[:, :nope].astype(bf16)
        qr[at(i), :] = (
            query[:, nope : nope + turn] * pcos_ref[at(i), :]
            + query[:, nope + turn :] * psin_ref[at(i), :]
        ).astype(bf16)
        expanded[at(i), :] = jnp.dot(
            latent(kv_chunks, kvgain_ref), kvup[...], preferred_element_type=f32
        ).astype(bf16)
        rope_key[at(i), :] = lat_all[0, rope_at[0], at(i), rope_at[1] : rope_at[1] + 128]
        return carry

    lax.fori_loop(0, n_sp, expand, 0)
    scale = (NOPE_DIM + ROPE_DIM) ** (-0.5)
    for b in range(n_sp):
        seen = (b + 1) * rows
        block = slice(b * rows, seen)
        q_at = lax.broadcasted_iota(jnp.int32, (rows, seen), 0) + b * rows
        k_at = lax.broadcasted_iota(jnp.int32, (rows, seen), 1)
        for h in range(att_heads):
            base = h * (NOPE_DIM + VAL_DIM)
            turned = qr[block, :]
            lane = lax.broadcasted_iota(jnp.int32, turned.shape, 1)
            turned = jnp.where(lane // ROPE_DIM == h, turned, jnp.zeros_like(turned))
            s = lax.dot_general(
                qn[block, h * NOPE_DIM : (h + 1) * NOPE_DIM],
                expanded[:seen, base : base + NOPE_DIM],
                CONTRACT,
                preferred_element_type=f32,
            ) + lax.dot_general(
                turned, rope_key[:seen, :], CONTRACT, preferred_element_type=f32
            )
            s = jnp.where(k_at <= q_at, s * scale, -jnp.inf)
            p = jnp.exp(s - jnp.max(s, axis=-1, keepdims=True))
            raw = jnp.dot(
                p.astype(bf16),
                expanded[:seen, base + NOPE_DIM : base + NOPE_DIM + VAL_DIM],
                preferred_element_type=f32,
            ) / jnp.sum(p, axis=-1, keepdims=True)
            scaled = raw * lax.rsqrt(jnp.mean(raw * raw, axis=-1, keepdims=True) + EPSILON)
            gain = again_ref[z][:, h * VAL_DIM : (h + 1) * VAL_DIM]
            merged[block, WIDE + h * VAL_DIM : WIDE + (h + 1) * VAL_DIM] = (
                scaled * gain
            ).astype(bf16)

    for d in range(n_sp):
        arrive(d, LATER)
    theirs = pl.ds(pl.multiple_of(other * half, half), half)
    pair_copies, row_copies = {}, {}
    order = list(range(1, n_sp)) + [0]
    for d in order:
        target = (z + d) % n_sp
        start = pl.multiple_of(target * rows, rows)
        for which in (theirs, mine):
            got = lax.dot_general(
                merged[pl.ds(pl.multiple_of(start + which.start, half), half), :],
                w_all[:, 4 * WIDE :],
                CONTRACT,
                preferred_element_type=f32,
            )
            if which is theirs:
                pair_out[d] = got.astype(bf16)
                pair_copies[d] = remote(
                    pair_out.at[d], pair_in.at[d], m_send.at[5, d], m_recv.at[5, d], tp=other
                )
                pair_copies[d].start()
            else:
                own_sum[d] = got
    for d in order:
        pair_copies[d].wait_recv()
        total = own_sum[d] + pair_in[d].astype(f32)
        if d:
            row_out[d] = total.astype(bf16)
            row_copies[d] = remote(
                row_out.at[d],
                row_in.at[d],
                m_send.at[6, d],
                m_recv.at[6, d],
                sp=(z + d) % n_sp,
            )
            row_copies[d].start()
        else:
            own_sum[0] = total
    total = own_sum[0]
    for d in range(1, n_sp):
        row_copies[d].wait_recv()
        total = total + row_in[d].astype(f32)
    out_ref[...] = total.astype(bf16)

    sent = pending + [c for group in (
        tok_copies, z_copies, x_copies, y_copies, f_copies, lat_copies, pair_copies, row_copies
    ) for c in group.values()]
    for copy in sent:
        copy.wait_send()


def heads_plan(
    tokens,
    norm_gain,
    w_ret_query,
    w_ret_key,
    w_ret_value,
    w_q_down,
    w_kv_down,
    w_rope_key,
    w_q_up,
    w_kv_up,
    q_lat_gain,
    kv_lat_gain,
    att_norm_gain,
    ret_norm_gain,
    w_ret_out,
    w_att_out,
    head_rate,
    decay_shift,
    start_state,
):
    n_sp = lax.axis_size("sp")
    z = lax.axis_index("sp")
    rows, width = tokens.shape[1:]
    length = n_sp * rows
    q_wide, kv_wide = w_q_down.shape[1], w_kv_down.shape[1]
    rope_half = ROPE_DIM // 2
    w_rows = w_q_down.shape[0]
    att_heads = w_q_up.shape[1] // (NOPE_DIM + ROPE_DIM) // n_sp

    def swap(x):
        return jnp.concatenate([x[..., rope_half:], x[..., :rope_half]], axis=-1)

    lat = jnp.concatenate([w_q_down, w_kv_down, w_rope_key, swap(w_rope_key)], axis=1)
    lat = jnp.pad(lat, ((0, 0), (0, n_sp * WIDE - lat.shape[1])))
    head_wide = NOPE_DIM + ROPE_DIM
    q_up = lax.dynamic_slice_in_dim(w_q_up, z * att_heads * head_wide, att_heads * head_wide, 1)
    q_up = q_up.reshape(-1, att_heads, head_wide)
    turned = q_up[..., NOPE_DIM:]
    q_up = jnp.concatenate(
        [a.reshape(a.shape[0], -1) for a in (q_up[..., :NOPE_DIM], turned, swap(turned))], axis=1
    )
    positions = jnp.arange(length, dtype=jnp.int32)
    ret_cos, ret_sin = angle_tables(positions, RET_DIM)
    rope_cos, rope_sin = angle_tables(positions, ROPE_DIM)
    pair_cos = jnp.concatenate([rope_cos] * 4, axis=1)
    pair_sin = jnp.concatenate([-rope_sin, rope_sin] * 2, axis=1)
    dma = pltpu.SemaphoreType.DMA
    vmem = pltpu.VMEM
    f32, bf16 = jnp.float32, jnp.bfloat16
    half = rows // 2
    out_wide = 4 * n_sp * w_rows
    any_spec = pl.BlockSpec(memory_space=pl.ANY)
    vmem_spec = pl.BlockSpec(memory_space=pltpu.VMEM)
    mixed = pl.pallas_call(
        functools.partial(layer_kernel, n_sp, q_wide, kv_wide),
        out_shape=jax.ShapeDtypeStruct((half, out_wide), bf16),
        in_specs=[any_spec] * 8 + [vmem_spec] * 11 + [any_spec] * 2,
        out_specs=vmem_spec,
        scratch_shapes=[
            vmem((n_sp, rows, width), bf16),
            vmem((n_sp * 4 * w_rows, 6 * WIDE), bf16),
            vmem((n_sp,) + decay_shift.shape[1:], f32),
            vmem((length, width), bf16),
            vmem((length, 4 * WIDE), f32),
            vmem((length, WIDE), bf16),
            vmem((length, WIDE), bf16),
            vmem((length, WIDE), bf16),
            vmem((2, n_sp, length, WIDE), bf16),
            vmem((RET_DIM, RET_DIM), f32),
            vmem((length, att_heads * NOPE_DIM), bf16),
            vmem((length, att_heads * ROPE_DIM), bf16),
            vmem((length, att_heads * (NOPE_DIM + VAL_DIM)), bf16),
            vmem((length, 2 * ROPE_DIM), bf16),
            vmem((w_kv_up.shape[0], att_heads * (NOPE_DIM + VAL_DIM)), bf16),
            vmem((length, WIDE + att_heads * VAL_DIM), bf16),
            vmem((n_sp, half, out_wide), f32),
            vmem((n_sp, half, out_wide), bf16),
            vmem((n_sp, half, out_wide), bf16),
            vmem((n_sp, half, out_wide), bf16),
            vmem((n_sp, half, out_wide), bf16),
            dma((10,)),
            dma((n_sp, 6)),
            dma((n_sp, 6)),
            dma((n_sp, 4)),
            dma((n_sp, 4)),
            dma((n_sp, 4)),
            dma((n_sp, 4)),
            dma((n_sp, 4)),
            dma((n_sp, 4)),
            dma((7, n_sp)),
            dma((7, n_sp)),
        ],
        compiler_params=pltpu.CompilerParams(
            collective_id=0, has_side_effects=True, vmem_limit_bytes=62 * 1024 * 1024
        ),
    )(
        tokens[0],
        lat,
        w_ret_query,
        w_ret_key,
        w_ret_value,
        w_ret_out,
        w_att_out,
        decay_shift[0],
        head_rate[:, None],
        norm_gain[None],
        q_lat_gain[None],
        kv_lat_gain[None],
        att_norm_gain.reshape(n_sp, 1, -1),
        ret_norm_gain.reshape(n_sp, 1, -1),
        ret_cos,
        ret_sin,
        pair_cos,
        pair_sin,
        q_up,
        w_kv_up,
        start_state[0],
    )
    return mixed[None]


def solution(mesh):
    placed = (
        P("fs", "sp", None),
        P(),
        P(("sp", "fs"), "tp"),
        P(("sp", "fs"), "tp"),
        P(("sp", "fs"), "tp"),
        P(("sp", "fs"), "tp"),
        P(("sp", "fs"), "tp"),
        P(("sp", "fs"), None),
        P(None, "tp"),
        P(None, "tp"),
        P(),
        P(),
        P("tp"),
        P("tp"),
        P(("sp", "fs"), "tp"),
        P(("sp", "fs"), "tp"),
        P("tp"),
        P("fs", "tp", "sp"),
        P("fs", "tp", None, None),
    )

    def pick(*args):
        if heads_fit(
            mesh, args[16].shape[0], args[0].shape[0], args[5].shape[1], args[6].shape[1]
        ):
            return heads_plan(*args)
        return rows_plan(*args)

    return jax.shard_map(
        pick,
        mesh=mesh,
        in_specs=placed,
        out_specs=P("fs", ("sp", "tp"), None),
        check_vma=False,
    )
```

```python
import functools

import numpy as np

import jax
import jax.numpy as jnp
from jax import lax
from jax.experimental import pallas as pl
from jax.experimental.pallas import tpu as pltpu
from jax.sharding import PartitionSpec as P

RET_DIM = 256
NOPE_DIM = 128
ROPE_DIM = 64
VAL_DIM = 128
KV_LAT = 512


EPSILON = 1e-06
THETA_BASE = 10000.0
TOP_PRECISION = lax.Precision.HIGHEST


def prefix(x, axis, combine, identity):
    peers, position = (lax.axis_size(axis), lax.axis_index(axis))
    everything = jax.tree.map(
        lambda part, kind: lax.all_gather(part.astype(kind), axis), x, (jnp.bfloat16, jnp.bfloat16)
    )
    start = jax.tree.map(
        lambda part, zero: jnp.broadcast_to(jnp.asarray(zero, part.dtype), part.shape), x, identity
    )

    def lap(k, before):
        reached = k < position
        new = combine(
            before, jax.tree.map(lambda part, own: part[k].astype(own.dtype), everything, x)
        )
        return jax.tree.map(lambda a, b: jnp.where(reached, a, b), new, before)

    return lax.fori_loop(0, peers, lap, start)


def angle_tables(positions, rot_width):
    half_width = rot_width // 2
    inverse = THETA_BASE ** (-jnp.arange(half_width, dtype=jnp.float32) * 2.0 / rot_width)
    angles = positions.astype(jnp.float32)[:, None] * inverse[None, :]
    return (jnp.cos(angles), jnp.sin(angles))


def rotate(values, cosine, sine):
    half_width = values.shape[-1] // 2
    front_half = values[..., :half_width]
    back_half = values[..., half_width:]
    return jnp.concatenate(
        [front_half * cosine - back_half * sine, back_half * cosine + front_half * sine], axis=-1
    )


def rms_scale(values, gain_vector):
    return (
        values
        * lax.rsqrt(jnp.mean(values * values, axis=-1, keepdims=True) + EPSILON)
        * gain_vector
    )


def chain_states(earlier, later):
    early_log, early_state = earlier
    late_log, late_state = later
    return (early_log + late_log, jnp.exp(late_log)[:, None, None] * early_state + late_state)


def rows_plan(
    tokens,
    norm_gain,
    w_ret_query,
    w_ret_key,
    w_ret_value,
    w_q_down,
    w_kv_down,
    w_rope_key,
    w_q_up,
    w_kv_up,
    q_lat_gain,
    kv_lat_gain,
    att_norm_gain,
    ret_norm_gain,
    w_ret_out,
    w_att_out,
    head_rate,
    decay_shift,
    start_state,
):
    tok_rows = tokens.shape[1]
    ret_local = head_rate.shape[0]
    att_local = w_q_up.shape[1] // (NOPE_DIM + ROPE_DIM)
    row_offset = lax.axis_index("sp") * tok_rows
    positions = row_offset + jnp.arange(tok_rows, dtype=jnp.int32)
    (
        full_query,
        full_key,
        full_value,
        full_q_down,
        full_kv_down,
        full_rope,
        full_ret_out,
        full_att_out,
    ) = (
        lax.all_gather(w_ret_query, ("sp", "fs"), axis=0, tiled=True),
        lax.all_gather(w_ret_key, ("sp", "fs"), axis=0, tiled=True),
        lax.all_gather(w_ret_value, ("sp", "fs"), axis=0, tiled=True),
        lax.all_gather(w_q_down, ("sp", "fs"), axis=0, tiled=True),
        lax.all_gather(w_kv_down, ("sp", "fs"), axis=0, tiled=True),
        lax.all_gather(w_rope_key, ("sp", "fs"), axis=0, tiled=True),
        lax.all_gather(w_ret_out, ("sp", "fs"), axis=0, tiled=True),
        lax.all_gather(w_att_out, ("sp", "fs"), axis=0, tiled=True),
    )
    source = tokens[0].astype(jnp.float32)
    normed = rms_scale(source, norm_gain).astype(jnp.bfloat16)
    ret_cos, ret_sin = angle_tables(positions, RET_DIM)
    rope_cos, rope_sin = angle_tables(positions, ROPE_DIM)

    def project(weight):
        return jnp.dot(normed, weight, preferred_element_type=jnp.float32)

    part_q = project(full_q_down).astype(jnp.bfloat16)
    part_kv = project(full_kv_down).astype(jnp.bfloat16)
    lat_q_raw, lat_kv_raw = (
        lax.all_gather(part_q, "tp", axis=1, tiled=True),
        lax.all_gather(part_kv, "tp", axis=1, tiled=True),
    )
    retention_query = rotate(
        project(full_query).reshape(tok_rows, ret_local, RET_DIM),
        ret_cos[:, None],
        ret_sin[:, None],
    ).astype(jnp.bfloat16)
    retention_key = (
        rotate(
            project(full_key).reshape(tok_rows, ret_local, RET_DIM),
            ret_cos[:, None],
            ret_sin[:, None],
        )
        * RET_DIM ** (-0.5)
    ).astype(jnp.bfloat16)
    retention_value = project(full_value).reshape(tok_rows, ret_local, RET_DIM).astype(jnp.bfloat16)
    rope_key = rotate(project(full_rope), rope_cos, rope_sin).astype(jnp.bfloat16)
    log_rates = head_rate[:, None] + decay_shift[0]
    cumul = jnp.cumsum(log_rates, axis=1)
    offsets = jnp.arange(tok_rows, dtype=jnp.int32)
    lower_mask = offsets[None, :] <= offsets[:, None]
    decay_matrix = jnp.exp(
        jnp.where(lower_mask[None], cumul[:, :, None] - cumul[:, None, :], -jnp.inf)
    )
    block_score_grid = (
        jnp.einsum(
            "zgq,ugq->gzu", retention_query, retention_key, preferred_element_type=jnp.float32
        )
        * decay_matrix
    ).astype(jnp.bfloat16)
    inside_block_output = jnp.einsum(
        "vzs,svp->zvp", block_score_grid, retention_value, preferred_element_type=jnp.float32
    )
    block_output_sum = cumul[:, -1]
    weighted_values = (
        retention_key.astype(jnp.float32) * jnp.exp(block_output_sum[:, None] - cumul).T[:, :, None]
    )
    contribution = jnp.einsum(
        "uzj,uzv->zjv",
        weighted_values,
        retention_value.astype(jnp.float32),
        precision=TOP_PRECISION,
    )
    identity = (jnp.zeros_like(block_output_sum), jnp.zeros_like(contribution))
    before_log, before_state = prefix(
        (block_output_sum, contribution), "sp", chain_states, identity
    )
    q_latent = rms_scale(lat_q_raw.astype(jnp.float32), q_lat_gain).astype(jnp.bfloat16)
    kv_latent = rms_scale(lat_kv_raw.astype(jnp.float32), kv_lat_gain).astype(jnp.bfloat16)
    query_full = jnp.dot(q_latent, w_q_up, preferred_element_type=jnp.float32).reshape(
        tok_rows, att_local, NOPE_DIM + ROPE_DIM
    )
    query_nope = query_full[..., :NOPE_DIM].astype(jnp.bfloat16)
    query_rope = rotate(query_full[..., NOPE_DIM:], rope_cos[:, None], rope_sin[:, None]).astype(
        jnp.bfloat16
    )
    att_scale = (NOPE_DIM + ROPE_DIM) ** (-0.5)

    def attend(carry, key_nope, key_values, key_rope, start):
        running_max, running_sum, running_acc = carry
        key_count = key_rope.shape[0]
        score_matrix = (
            jnp.einsum("qhd,khd->hqk", query_nope, key_nope, preferred_element_type=jnp.float32)
            + jnp.einsum("qhd,kd->hqk", query_rope, key_rope, preferred_element_type=jnp.float32)
        ) * att_scale
        key_positions = start + jnp.arange(key_count, dtype=jnp.int32)
        allowed = key_positions[None, :] <= positions[:, None]
        masked = jnp.where(allowed[None], score_matrix, -jnp.inf)
        new_max = jnp.maximum(running_max, jnp.max(masked, axis=-1))
        safe_max = jnp.where(jnp.isfinite(new_max), new_max, 0.0)
        weights = jnp.exp(masked - safe_max[..., None])
        rescale = jnp.exp(running_max - safe_max)
        new_sum = running_sum * rescale + jnp.sum(weights, axis=-1)
        new_acc = running_acc * rescale[..., None] + jnp.einsum(
            "hqk,khd->hqd",
            weights.astype(jnp.bfloat16),
            key_values,
            preferred_element_type=jnp.float32,
        )
        return (new_max, new_sum, new_acc)

    def expand_attend(carry_in, lat_piece, rope_piece, start):
        wide = (
            jnp.dot(lat_piece, w_kv_up, preferred_element_type=jnp.float32)
            .astype(jnp.bfloat16)
            .reshape(rope_piece.shape[0], att_local, NOPE_DIM + VAL_DIM)
        )
        return attend(carry_in, wide[..., :NOPE_DIM], wide[..., NOPE_DIM:], rope_piece, start)

    empty = (
        jnp.full((att_local, tok_rows), -jnp.inf, jnp.float32),
        jnp.zeros((att_local, tok_rows), jnp.float32),
        jnp.zeros((att_local, tok_rows, VAL_DIM), jnp.float32),
    )
    groups = lax.axis_size("tp")
    kv_part = KV_LAT // groups
    rope_part = ROPE_DIM // groups
    my_group = lax.axis_index("tp")
    joined = jnp.concatenate(
        [
            lax.dynamic_slice_in_dim(kv_latent, my_group * kv_part, kv_part, 1),
            lax.dynamic_slice_in_dim(rope_key, my_group * rope_part, rope_part, 1),
        ],
        axis=1,
    )
    all_rows = lax.all_gather(joined, "sp", axis=0, tiled=True)
    complete = lax.all_gather(all_rows, "tp", axis=1, tiled=True)
    total_rows = complete.shape[0]
    grouped = complete.reshape(total_rows, groups, kv_part + rope_part)
    lat_all = grouped[:, :, :kv_part].reshape(total_rows, KV_LAT)
    rope_all = grouped[:, :, kv_part:].reshape(total_rows, ROPE_DIM)

    def visit(block_index, carry_in):
        start = block_index * tok_rows
        lat_piece = lax.dynamic_slice_in_dim(lat_all, start, tok_rows, 0)
        rope_piece = lax.dynamic_slice_in_dim(rope_all, start, tok_rows, 0)
        return expand_attend(carry_in, lat_piece, rope_piece, start)

    final = lax.fori_loop(0, lax.axis_index("sp") + 1, visit, empty)
    att_raw = jnp.transpose(final[2] / final[1][..., None], (1, 0, 2))
    att_out = (
        rms_scale(att_raw, att_norm_gain.reshape(att_local, VAL_DIM))
        .astype(jnp.bfloat16)
        .reshape(tok_rows, att_local * VAL_DIM)
    )
    entering = jnp.exp(before_log)[:, None, None] * start_state[0] + before_state
    carried_term = (
        jnp.einsum(
            "nhd,hde->nhe", retention_query.astype(jnp.float32), entering, precision=TOP_PRECISION
        )
        * jnp.exp(cumul).T[:, :, None]
    )
    ret_raw = inside_block_output + carried_term
    row_mean = jnp.mean(ret_raw, axis=-1, keepdims=True)
    centered = ret_raw - row_mean
    row_var = jnp.mean(centered * centered, axis=-1, keepdims=True)
    ret_out = (
        (centered * lax.rsqrt(row_var + EPSILON) * ret_norm_gain.reshape(ret_local, RET_DIM))
        .astype(jnp.bfloat16)
        .reshape(tok_rows, ret_local * RET_DIM)
    )
    contract = (((1,), (1,)), ((), ()))
    mixed = lax.psum_scatter(
        (
            lax.dot_general(ret_out, full_ret_out, contract, preferred_element_type=jnp.float32)
            + lax.dot_general(att_out, full_att_out, contract, preferred_element_type=jnp.float32)
        ).astype(jnp.bfloat16),
        "tp",
        scatter_dimension=0,
        tiled=True,
    )
    return mixed[None]


MESH = pl.DeviceIdType.MESH
WIDE = RET_DIM
CONTRACT = (((1,), (1,)), ((), ()))
GROUPS = ((0, 2), (2, 2), (4, 1), (5, 1))
FIRST, LATER = (0, 1), (2, 3)


def heads_fit(mesh, ret_local, sequences, q_wide, kv_wide, up_wide):
    sizes = mesh.shape
    return (
        sizes["sp"] == 4
        and sizes["fs"] == 4
        and sizes["tp"] == 2
        and ret_local == sizes["sp"]
        and sequences == 1
        and up_wide == 2 * (NOPE_DIM + ROPE_DIM) * ret_local
        and q_wide % 128 == 0
        and kv_wide % 128 == 0
        and q_wide + kv_wide + 2 * ROPE_DIM <= ret_local * WIDE
    )


def wave_tables(length, wide):
    half_wide = wide // 2
    powers = np.arange(half_wide, dtype=np.float32) * np.float32(2.0 / wide)
    inverse = np.power(np.float32(THETA_BASE), -powers).astype(np.float32)
    angles = np.arange(length, dtype=np.float32)[:, None] * inverse[None, :]
    return np.cos(angles), np.sin(angles)


def three_parts(x):
    high = x.astype(jnp.bfloat16)
    rest = x - high.astype(jnp.float32)
    middle = rest.astype(jnp.bfloat16)
    low = (rest - middle.astype(jnp.float32)).astype(jnp.bfloat16)
    return high, middle, low


def layer_kernel(
    n_sp,
    q_wide,
    kv_wide,
    tok_ref,
    lat_ref,
    wq_ref,
    wk_ref,
    wv_ref,
    wr_ref,
    wa_ref,
    shift_ref,
    rate_ref,
    gain_ref,
    qgain_ref,
    kvgain_ref,
    again_ref,
    rgain_ref,
    rcos_ref,
    rsin_ref,
    pcos_ref,
    psin_ref,
    qup_ref,
    kvup_ref,
    start_ref,
    out_ref,
    tok_all,
    w_all,
    shift_all,
    normed,
    acc,
    ret_q,
    ret_k,
    ret_v,
    lat_all,
    state,
    qn,
    qr,
    expanded,
    rope_key,
    kvup,
    qup,
    merged,
    own_sum,
    pair_out,
    pair_in,
    row_out,
    row_in,
    local_sem,
    z_send,
    z_recv,
    x_send,
    x_recv,
    y_send,
    y_recv,
    f_send,
    f_recv,
    m_send,
    m_recv,
    l_send,
    l_recv,
    l_relay,
    p_send,
    p_recv,
):
    z, f, t = lax.axis_index("sp"), lax.axis_index("fs"), lax.axis_index("tp")
    xn = f + 1 - 2 * (f % 2)
    yn = (f + 2) % 4
    other = 1 - t
    fs = 4
    rows = tok_ref.shape[0]
    half = rows // 2
    weights = (lat_ref, wq_ref, wk_ref, wv_ref, wr_ref, wa_ref)
    f32, bf16 = jnp.float32, jnp.bfloat16

    def remote(src, dst, send, recv, **where):
        return pltpu.make_async_remote_copy(
            src_ref=src,
            dst_ref=dst,
            send_sem=send,
            recv_sem=recv,
            device_id={"sp": z, "fs": f, "tp": t, **where},
            device_id_type=MESH,
        )

    barrier = pltpu.get_barrier_semaphore()
    peers = [{"sp": (z + d) % n_sp, "fs": f, "tp": t} for d in range(1, n_sp)]
    peers += [{"sp": z, "fs": xn, "tp": t}, {"sp": z, "fs": yn, "tp": t}]
    peers += [{"sp": z, "fs": f, "tp": other}]
    for peer in peers:
        pl.semaphore_signal(barrier, inc=1, device_id=peer, device_id_type=MESH)
    pl.semaphore_wait(barrier, len(peers))

    def piece(u, owner):
        return weights[u].at[:, pl.ds(pl.multiple_of(owner * WIDE, WIDE), WIDE)]

    def part(owner_z, owner_f, g):
        first, count = GROUPS[g]
        start = pl.multiple_of((owner_z * fs + owner_f) * rows, rows)
        return w_all.at[pl.ds(start, rows), pl.ds(first * WIDE, count * WIDE)]

    def unit(u):
        start = pl.multiple_of((z * fs + f) * rows, rows)
        return w_all.at[pl.ds(start, rows), pl.ds(u * WIDE, WIDE)]

    pending = []

    def go(copy):
        copy.start()
        pending.append(copy)
        return copy

    def owner(d):
        return (z + n_sp - d) % n_sp

    mine = pl.ds(pl.multiple_of(t * half, half), half)
    z_copies, x_copies, y_copies, f_copies = {}, {}, {}, {}

    def tok_part(origin):
        return tok_all.at[origin, mine]

    def lat_part(i):
        return lambda origin: lat_all.at[t, origin, pl.ds(i * rows, rows)]

    def direct(dest):
        near = (z - dest == 1) | (dest - z == 1)
        return near if dest in (0, n_sp - 1) else z != dest

    def line_copy(where, row, dest, src=None):
        return remote(
            where(z) if src is None else src,
            where(z),
            l_send.at[row, dest],
            l_recv.at[row, z],
            sp=dest,
        )

    def relay_copy(where, row, origin, dest):
        ref = where(origin)
        return remote(ref, ref, l_relay.at[row, origin], l_recv.at[row, origin], sp=dest)

    def pair_copy(where, row, origin):
        ref = where(origin)
        return remote(ref, ref, p_send.at[row, origin], p_recv.at[row, origin], tp=other)

    def line_start(where, row, src=None, pair=True):
        for dest in range(n_sp):
            pl.when(direct(dest))(lambda dest=dest: line_copy(where, row, dest, src).start())
        if pair:
            for origin in range(n_sp):
                pl.when(origin == z)(
                    lambda origin=origin: pair_copy(where, row, origin).start()
                )

    def passes_on(origin):
        if origin < n_sp // 2:
            return z == n_sp - 2, n_sp - 1
        return z == 1, 0

    def line_pass(where, row):
        for origin in range(n_sp):

            @pl.when(origin != z)
            def _(origin=origin):
                relay_copy(where, row, origin, 0).wait_recv()
                should, dest = passes_on(origin)
                pl.when(should)(lambda: relay_copy(where, row, origin, dest).start())
                pair_copy(where, row, origin).start()

    def pair_arrive(where, row, own):
        for origin in range(n_sp):
            if own:
                pair_copy(where, row, origin).wait_recv()
            else:
                pl.when(origin != z)(
                    lambda origin=origin: pair_copy(where, row, origin).wait_recv()
                )

    def line_drain(where, row, own):
        for other_z in range(n_sp):
            pl.when(direct(other_z))(
                lambda dest=other_z: line_copy(where, row, dest).wait_send()
            )
            if own:
                pair_copy(where, row, other_z).wait_send()

            @pl.when(other_z != z)
            def _(origin=other_z):
                should, dest = passes_on(origin)
                pl.when(should)(lambda: relay_copy(where, row, origin, dest).wait_send())
                if not own:
                    pair_copy(where, row, origin).wait_send()

    line_start(tok_part, 0, tok_ref.at[mine], pair=False)
    for d in range(1, n_sp):
        to = (z + d) % n_sp
        go(remote(shift_ref, shift_all.at[z], m_send.at[2, d], m_recv.at[2, d], sp=to))
    shift_copies = list(pending)
    pending.clear()
    locals_ = []
    for u in range(6):
        copy = pltpu.make_async_copy(piece(u, z), unit(u), local_sem.at[u])
        copy.start()
        locals_.append(copy)
    own_tok = pltpu.make_async_copy(tok_ref, tok_all.at[z], local_sem.at[6])
    own_tok.start()
    own_shift = pltpu.make_async_copy(shift_ref, shift_all.at[z], local_sem.at[7])
    own_shift.start()
    att_wide = kvup.shape[1]
    own_kvup = pltpu.make_async_copy(
        kvup_ref.at[:, pl.ds(pl.multiple_of(z * att_wide, att_wide), att_wide)],
        kvup,
        local_sem.at[8],
    )
    own_kvup.start()
    up_wide = qup.shape[1]
    own_qup = pltpu.make_async_copy(
        qup_ref.at[:, pl.ds(pl.multiple_of(z * up_wide, up_wide), up_wide)],
        qup,
        local_sem.at[10],
    )
    own_qup.start()
    own_state = pltpu.make_async_copy(start_ref.at[z], state, local_sem.at[9])
    own_state.start()
    for group in (FIRST, LATER):
        for d in range(1, n_sp):
            to = (z + d) % n_sp
            for g in group:
                for u in range(GROUPS[g][0], sum(GROUPS[g])):
                    z_copies[d, u] = remote(
                        piece(u, to), unit(u), z_send.at[d, u], z_recv.at[d, u], sp=to
                    )
                    z_copies[d, u].start()

    def spread(d, group):
        for g in group:
            for u in range(GROUPS[g][0], sum(GROUPS[g])):
                if d == 0:
                    locals_[u].wait()
                else:
                    z_copies[d, u].wait_recv()
            ref = part(owner(d), f, g)
            x_copies[d, g] = remote(ref, ref, x_send.at[d, g], x_recv.at[d, g], fs=xn)
            y_copies[d, g] = remote(ref, ref, y_send.at[d, g], y_recv.at[d, g], fs=yn)
            x_copies[d, g].start()
            y_copies[d, g].start()

    def relay(d, group):
        for g in group:
            if g % 2 == 0:
                x_copies[d, g].wait_recv()
                ref, to = part(owner(d), xn, g), yn
            else:
                y_copies[d, g].wait_recv()
                ref, to = part(owner(d), yn, g), xn
            f_copies[d, g] = remote(ref, ref, f_send.at[d, g], f_recv.at[d, g], fs=to)
            f_copies[d, g].start()

    def arrive(d, group):
        for g in group:
            if g % 2 == 0:
                y_copies[d, g].wait_recv()
            else:
                x_copies[d, g].wait_recv()
            f_copies[d, g].wait_recv()

    def at(i):
        if isinstance(i, int):
            return slice(i * rows, (i + 1) * rows)
        return pl.ds(pl.multiple_of(i * rows, rows), rows)

    def norm_block(i):
        x = tok_all[i].astype(f32)
        scaled = x * lax.rsqrt(jnp.mean(x * x, axis=-1, keepdims=True) + EPSILON)
        normed[at(i), :] = (scaled * gain_ref[...]).astype(bf16)

    spread(0, FIRST)
    own_tok.wait()
    norm_block(z)
    line_pass(tok_part, 0)
    for d in range(1, n_sp):
        spread(d, FIRST)
        relay(d - 1, FIRST)
        if d == 1:
            pair_arrive(tok_part, 0, False)
        norm_block(owner(d))
    relay(n_sp - 1, FIRST)
    spread(0, LATER)
    depth = fs * rows
    for d in range(n_sp):
        arrive(d, FIRST)
        begin = pl.multiple_of(owner(d) * depth, depth)

        def multiply(i, carry, d=d, begin=begin):
            got = jnp.dot(
                normed[at(i), pl.ds(begin, depth)],
                w_all[pl.ds(begin, depth), : 4 * WIDE],
                preferred_element_type=f32,
            )
            if d == 0:
                acc[at(i), :] = got
            else:
                acc[at(i), :] += got
            return carry

        lax.fori_loop(0, n_sp, multiply, 0)

    rope_index = (q_wide + kv_wide) // WIDE
    rope_lane = (q_wide + kv_wide) % WIDE
    rd = RET_DIM // 2

    def finish_lat(i, carry):
        raw = acc[at(i), :WIDE]
        pair = raw[:, rope_lane : rope_lane + 2 * ROPE_DIM]
        turned = pair * pcos_ref[at(i), :] + pltpu.roll(pair, ROPE_DIM, 1) * psin_ref[at(i), :]
        lane = lax.broadcasted_iota(jnp.int32, turned.shape, 1)
        turned = jnp.where(lane < ROPE_DIM, turned, pltpu.roll(turned, ROPE_DIM, 1))
        pieces = [raw[:, :rope_lane]] if rope_lane else []
        pieces.append(jnp.where(z == rope_index, turned, pair))
        if rope_lane + 2 * ROPE_DIM < WIDE:
            pieces.append(raw[:, rope_lane + 2 * ROPE_DIM :])
        lat_all[t, z, at(i), :] = jnp.concatenate(pieces, axis=1).astype(bf16)
        return carry

    for i in range(n_sp):
        finish_lat(i, 0)
        line_start(lat_part(i), i + 1)

    def finish_ret(i, carry):
        cosine, sine = rcos_ref[at(i), :], rsin_ref[at(i), :]
        for dst, base, factor in ((ret_q, WIDE, 1.0), (ret_k, 2 * WIDE, RET_DIM ** (-0.5))):
            a, b = acc[at(i), base : base + rd], acc[at(i), base + rd : base + WIDE]
            dst[at(i), :rd] = ((a * cosine - b * sine) * factor).astype(bf16)
            dst[at(i), rd:] = ((b * cosine + a * sine) * factor).astype(bf16)
        ret_v[at(i), :] = acc[at(i), 3 * WIDE :].astype(bf16)
        return carry

    lax.fori_loop(0, n_sp, finish_ret, 0)

    for copy in shift_copies:
        copy.wait()
    own_shift.wait()
    own_state.wait()
    r_iota = lax.broadcasted_iota(jnp.int32, (rows, rows), 0)
    c_iota = lax.broadcasted_iota(jnp.int32, (rows, rows), 1)

    def retention(b):
        rates = shift_all[b]
        pick = lax.broadcasted_iota(jnp.int32, rates.shape, 0) == z
        chosen = lax.broadcasted_iota(jnp.int32, rate_ref.shape, 1) == z
        rate = jnp.sum(jnp.where(chosen, rate_ref[...], 0.0), axis=1, keepdims=True)
        row = jnp.sum(jnp.where(pick, rates, 0.0), axis=0, keepdims=True) + rate
        column = jnp.sum(jnp.where(r_iota == c_iota, row, 0.0), axis=1, keepdims=True)
        c_col = jnp.sum(jnp.where(c_iota <= r_iota, row, 0.0), axis=1, keepdims=True)
        c_row = jnp.sum(jnp.where(r_iota <= c_iota, column, 0.0), axis=0, keepdims=True)
        last = jnp.sum(row, axis=1, keepdims=True)
        decay = jnp.exp(jnp.where(c_iota <= r_iota, c_col - c_row, -jnp.inf))
        block = slice(b * rows, (b + 1) * rows)
        q, k, v = ret_q[block, :], ret_k[block, :], ret_v[block, :]
        scores = lax.dot_general(q, k, CONTRACT, preferred_element_type=f32) * decay
        raw = jnp.dot(scores.astype(bf16), v, preferred_element_type=f32)
        carried = sum(
            jnp.dot(q, s, preferred_element_type=f32) for s in three_parts(state[...])
        )
        raw = raw + carried * jnp.exp(c_col)
        if b < n_sp - 1:
            weighted = k.astype(f32) * jnp.exp(last - c_col)
            added = sum(
                lax.dot_general(w, v, (((0,), (0,)), ((), ())), preferred_element_type=f32)
                for w in three_parts(weighted)
            )
            state[...] = jnp.exp(last) * state[...] + added
        centered = raw - jnp.mean(raw, axis=-1, keepdims=True)
        variance = jnp.mean(centered * centered, axis=-1, keepdims=True)
        merged[block, :WIDE] = (centered * lax.rsqrt(variance + EPSILON) * rgain_ref[z]).astype(
            bf16
        )

    for b in range(n_sp):
        if b:
            spread(b, LATER)
            relay(b - 1, LATER)
        line_pass(lat_part(b), b + 1)
        retention(b)
    relay(n_sp - 1, LATER)
    own_kvup.wait()
    own_qup.wait()

    def chunks(first, count):
        found = []
        for core in range(2):
            for j in range(count // 128):
                lane = first + j * 128
                found.append((core, lane // WIDE, lane % WIDE))
        return found

    q_chunks, kv_chunks = chunks(0, q_wide), chunks(q_wide, kv_wide)
    rope_at = (rope_index, rope_lane)
    att_heads = att_wide // (NOPE_DIM + VAL_DIM)
    nope = att_heads * NOPE_DIM
    turn = att_heads * ROPE_DIM

    def expand(i, carry):
        def latent(found, gain):
            x = jnp.concatenate(
                [lat_all[c, s, at(i), lane : lane + 128] for c, s, lane in found], axis=1
            ).astype(f32)
            scaled = x * lax.rsqrt(jnp.mean(x * x, axis=-1, keepdims=True) + EPSILON)
            return (scaled * gain[...]).astype(bf16)

        query = jnp.dot(latent(q_chunks, qgain_ref), qup[...], preferred_element_type=f32)
        first, middle, end = query[:, :128], query[:, 128:256], query[:, 256:]
        lane = lax.broadcasted_iota(jnp.int32, first.shape, 1)
        second = jnp.where(
            lane < ROPE_DIM, pltpu.roll(middle, ROPE_DIM, 1), pltpu.roll(end, ROPE_DIM, 1)
        )
        pair = jnp.where(lane < ROPE_DIM, middle, end)
        quarter = ROPE_DIM // 2
        swapped = jnp.where(
            lane % ROPE_DIM < quarter,
            pltpu.roll(pair, 2 * ROPE_DIM - quarter, 1),
            pltpu.roll(pair, quarter, 1),
        )
        qn[at(i), :NOPE_DIM] = first.astype(bf16)
        qn[at(i), NOPE_DIM:] = second.astype(bf16)
        qr[at(i), :] = (pair * pcos_ref[at(i), :] + swapped * psin_ref[at(i), :]).astype(bf16)
        expanded[at(i), :] = jnp.dot(
            latent(kv_chunks, kvgain_ref), kvup[...], preferred_element_type=f32
        ).astype(bf16)
        rope_key[at(i), :] = lat_all[0, rope_at[0], at(i), rope_at[1] : rope_at[1] + 128]
        return carry

    for i in range(n_sp):
        pair_arrive(lat_part(i), i + 1, True)
        expand(i, 0)
    for d in range(n_sp):
        arrive(d, LATER)
    theirs = pl.ds(pl.multiple_of(other * half, half), half)
    pair_copies = {}

    def row_copy(b, origin):
        return remote(row_out.at[b], row_in.at[origin], m_send.at[6, b], m_recv.at[6, origin], sp=b)

    def project_out(b):
        for which in (theirs, mine):
            start = pl.multiple_of(b * rows + which.start, half)
            got = lax.dot_general(
                merged[pl.ds(start, half), :],
                w_all[:, 4 * WIDE :],
                CONTRACT,
                preferred_element_type=f32,
            )
            if which is theirs:
                pair_out[b] = got.astype(bf16)
                pair_copies[b] = remote(
                    pair_out.at[b], pair_in.at[b], m_send.at[5, b], m_recv.at[5, b], tp=other
                )
                pair_copies[b].start()
            else:
                own_sum[b] = got

    def send_rows(b):
        pair_copies[b].wait_recv()
        total = own_sum[b] + pair_in[b].astype(f32)
        own_sum[b] = total

        @pl.when(z != b)
        def _():
            row_out[b] = total.astype(bf16)
            row_copy(b, z).start()

    scale = (NOPE_DIM + ROPE_DIM) ** (-0.5)
    order = (0, n_sp - 1) + tuple(range(1, n_sp - 1))
    for step, b in enumerate(order):
        seen = (b + 1) * rows
        block = slice(b * rows, seen)
        q_at = lax.broadcasted_iota(jnp.int32, (rows, seen), 0) + b * rows
        k_at = lax.broadcasted_iota(jnp.int32, (rows, seen), 1)
        for h in range(att_heads):
            base = h * (NOPE_DIM + VAL_DIM)
            turned = qr[block, :]
            lane = lax.broadcasted_iota(jnp.int32, turned.shape, 1)
            turned = jnp.where(lane // ROPE_DIM == h, turned, jnp.zeros_like(turned))
            s = lax.dot_general(
                qn[block, h * NOPE_DIM : (h + 1) * NOPE_DIM],
                expanded[:seen, base : base + NOPE_DIM],
                CONTRACT,
                preferred_element_type=f32,
            ) + lax.dot_general(
                turned, rope_key[:seen, :], CONTRACT, preferred_element_type=f32
            )
            s = jnp.where(k_at <= q_at, s * scale, -jnp.inf)
            p = jnp.exp(s - jnp.max(s, axis=-1, keepdims=True))
            raw = jnp.dot(
                p.astype(bf16),
                expanded[:seen, base + NOPE_DIM : base + NOPE_DIM + VAL_DIM],
                preferred_element_type=f32,
            ) / jnp.sum(p, axis=-1, keepdims=True)
            scaled = raw * lax.rsqrt(jnp.mean(raw * raw, axis=-1, keepdims=True) + EPSILON)
            gain = again_ref[z][:, h * VAL_DIM : (h + 1) * VAL_DIM]
            merged[block, WIDE + h * VAL_DIM : WIDE + (h + 1) * VAL_DIM] = (
                scaled * gain
            ).astype(bf16)

        project_out(b)
        if step:
            send_rows(order[step - 1])
    send_rows(order[-1])
    total = own_sum[z]
    for d in range(1, n_sp):
        row_copy(0, owner(d)).wait_recv()
        total = total + row_in[owner(d)].astype(f32)
    out_ref[...] = total.astype(bf16)

    for group in (z_copies, x_copies, y_copies, f_copies, pair_copies):
        for copy in group.values():
            copy.wait_send()
    line_drain(tok_part, 0, False)
    for i in range(n_sp):
        line_drain(lat_part(i), i + 1, True)
    for b in range(n_sp):
        pl.when(z != b)(lambda b=b: row_copy(b, z).wait_send())


def heads_plan(
    tokens,
    norm_gain,
    w_ret_query,
    w_ret_key,
    w_ret_value,
    w_q_down,
    w_kv_down,
    w_rope_key,
    w_q_up,
    w_kv_up,
    q_lat_gain,
    kv_lat_gain,
    att_norm_gain,
    ret_norm_gain,
    w_ret_out,
    w_att_out,
    head_rate,
    decay_shift,
    start_state,
):
    n_sp = lax.axis_size("sp")
    rows, width = tokens.shape[1:]
    length = n_sp * rows
    q_wide, kv_wide = w_q_down.shape[1], w_kv_down.shape[1]
    rope_half = ROPE_DIM // 2
    w_rows = w_q_down.shape[0]
    att_heads = w_q_up.shape[1] // (NOPE_DIM + ROPE_DIM) // n_sp

    def swap(x):
        return jnp.concatenate([x[..., rope_half:], x[..., :rope_half]], axis=-1)

    lat = jnp.concatenate([w_q_down, w_kv_down, w_rope_key, swap(w_rope_key)], axis=1)
    lat = jnp.pad(lat, ((0, 0), (0, n_sp * WIDE - lat.shape[1])))
    ret_cos, ret_sin = wave_tables(length, RET_DIM)
    rope_cos, rope_sin = wave_tables(length, ROPE_DIM)
    pair_cos = np.concatenate([rope_cos] * 4, axis=1)
    pair_sin = np.concatenate([-rope_sin, rope_sin] * 2, axis=1)
    dma = pltpu.SemaphoreType.DMA
    vmem = pltpu.VMEM
    f32, bf16 = jnp.float32, jnp.bfloat16
    half = rows // 2
    out_wide = 4 * n_sp * w_rows
    any_spec = pl.BlockSpec(memory_space=pl.ANY)
    vmem_spec = pl.BlockSpec(memory_space=pltpu.VMEM)
    mixed = pl.pallas_call(
        functools.partial(layer_kernel, n_sp, q_wide, kv_wide),
        out_shape=jax.ShapeDtypeStruct((half, out_wide), bf16),
        in_specs=[any_spec] * 8 + [vmem_spec] * 10 + [any_spec] * 3,
        out_specs=vmem_spec,
        scratch_shapes=[
            vmem((n_sp, rows, width), bf16),
            vmem((n_sp * 4 * w_rows, 6 * WIDE), bf16),
            vmem((n_sp,) + decay_shift.shape[1:], f32),
            vmem((length, width), bf16),
            vmem((length, 4 * WIDE), f32),
            vmem((length, WIDE), bf16),
            vmem((length, WIDE), bf16),
            vmem((length, WIDE), bf16),
            vmem((2, n_sp, length, WIDE), bf16),
            vmem((RET_DIM, RET_DIM), f32),
            vmem((length, att_heads * NOPE_DIM), bf16),
            vmem((length, att_heads * ROPE_DIM), bf16),
            vmem((length, att_heads * (NOPE_DIM + VAL_DIM)), bf16),
            vmem((length, 2 * ROPE_DIM), bf16),
            vmem((w_kv_up.shape[0], att_heads * (NOPE_DIM + VAL_DIM)), bf16),
            vmem((w_q_up.shape[0], att_heads * (NOPE_DIM + ROPE_DIM)), bf16),
            vmem((length, WIDE + att_heads * VAL_DIM), bf16),
            vmem((n_sp, half, out_wide), f32),
            vmem((n_sp, half, out_wide), bf16),
            vmem((n_sp, half, out_wide), bf16),
            vmem((n_sp, half, out_wide), bf16),
            vmem((n_sp, half, out_wide), bf16),
            dma((11,)),
            dma((n_sp, 6)),
            dma((n_sp, 6)),
            dma((n_sp, 4)),
            dma((n_sp, 4)),
            dma((n_sp, 4)),
            dma((n_sp, 4)),
            dma((n_sp, 4)),
            dma((n_sp, 4)),
            dma((7, n_sp)),
            dma((7, n_sp)),
            dma((n_sp + 1, n_sp)),
            dma((n_sp + 1, n_sp)),
            dma((n_sp + 1, n_sp)),
            dma((n_sp + 1, n_sp)),
            dma((n_sp + 1, n_sp)),
        ],
        compiler_params=pltpu.CompilerParams(
            collective_id=0, has_side_effects=True, vmem_limit_bytes=62 * 1024 * 1024
        ),
    )(
        tokens[0],
        lat,
        w_ret_query,
        w_ret_key,
        w_ret_value,
        w_ret_out,
        w_att_out,
        decay_shift[0],
        head_rate[None],
        norm_gain[None],
        q_lat_gain[None],
        kv_lat_gain[None],
        att_norm_gain.reshape(n_sp, 1, -1),
        ret_norm_gain.reshape(n_sp, 1, -1),
        ret_cos,
        ret_sin,
        pair_cos,
        pair_sin,
        w_q_up,
        w_kv_up,
        start_state[0],
    )
    return mixed[None]


def solution(mesh):
    placed = (
        P("fs", "sp", None),
        P(),
        P(("sp", "fs"), "tp"),
        P(("sp", "fs"), "tp"),
        P(("sp", "fs"), "tp"),
        P(("sp", "fs"), "tp"),
        P(("sp", "fs"), "tp"),
        P(("sp", "fs"), None),
        P(None, "tp"),
        P(None, "tp"),
        P(),
        P(),
        P("tp"),
        P("tp"),
        P(("sp", "fs"), "tp"),
        P(("sp", "fs"), "tp"),
        P("tp"),
        P("fs", "tp", "sp"),
        P("fs", "tp", None, None),
    )

    def pick(*args):
        if heads_fit(
            mesh, args[16].shape[0], args[0].shape[0], args[5].shape[1], args[6].shape[1], args[8].shape[1]
        ):
            return heads_plan(*args)
        return rows_plan(*args)

    return jax.shard_map(
        pick,
        mesh=mesh,
        in_specs=placed,
        out_specs=P("fs", ("sp", "tp"), None),
        check_vma=False,
    )
```

```python
import functools

import numpy as np

import jax
import jax.numpy as jnp
from jax import lax
from jax.experimental import pallas as pl
from jax.experimental.pallas import tpu as pltpu
from jax.sharding import PartitionSpec as P

RET_DIM = 256
NOPE_DIM = 128
ROPE_DIM = 64
VAL_DIM = 128
KV_LAT = 512


EPSILON = 1e-06
THETA_BASE = 10000.0
TOP_PRECISION = lax.Precision.HIGHEST


def prefix(x, axis, combine, identity):
    peers, position = (lax.axis_size(axis), lax.axis_index(axis))
    everything = jax.tree.map(
        lambda part, kind: lax.all_gather(part.astype(kind), axis), x, (jnp.bfloat16, jnp.bfloat16)
    )
    start = jax.tree.map(
        lambda part, zero: jnp.broadcast_to(jnp.asarray(zero, part.dtype), part.shape), x, identity
    )

    def lap(k, before):
        reached = k < position
        new = combine(
            before, jax.tree.map(lambda part, own: part[k].astype(own.dtype), everything, x)
        )
        return jax.tree.map(lambda a, b: jnp.where(reached, a, b), new, before)

    return lax.fori_loop(0, peers, lap, start)


def angle_tables(positions, rot_width):
    half_width = rot_width // 2
    inverse = THETA_BASE ** (-jnp.arange(half_width, dtype=jnp.float32) * 2.0 / rot_width)
    angles = positions.astype(jnp.float32)[:, None] * inverse[None, :]
    return (jnp.cos(angles), jnp.sin(angles))


def rotate(values, cosine, sine):
    half_width = values.shape[-1] // 2
    front_half = values[..., :half_width]
    back_half = values[..., half_width:]
    return jnp.concatenate(
        [front_half * cosine - back_half * sine, back_half * cosine + front_half * sine], axis=-1
    )


def rms_scale(values, gain_vector):
    return (
        values
        * lax.rsqrt(jnp.mean(values * values, axis=-1, keepdims=True) + EPSILON)
        * gain_vector
    )


def chain_states(earlier, later):
    early_log, early_state = earlier
    late_log, late_state = later
    return (early_log + late_log, jnp.exp(late_log)[:, None, None] * early_state + late_state)


def rows_plan(
    tokens,
    norm_gain,
    w_ret_query,
    w_ret_key,
    w_ret_value,
    w_q_down,
    w_kv_down,
    w_rope_key,
    w_q_up,
    w_kv_up,
    q_lat_gain,
    kv_lat_gain,
    att_norm_gain,
    ret_norm_gain,
    w_ret_out,
    w_att_out,
    head_rate,
    decay_shift,
    start_state,
):
    tok_rows = tokens.shape[1]
    ret_local = head_rate.shape[0]
    att_local = w_q_up.shape[1] // (NOPE_DIM + ROPE_DIM)
    row_offset = lax.axis_index("sp") * tok_rows
    positions = row_offset + jnp.arange(tok_rows, dtype=jnp.int32)
    (
        full_query,
        full_key,
        full_value,
        full_q_down,
        full_kv_down,
        full_rope,
        full_ret_out,
        full_att_out,
    ) = (
        lax.all_gather(w_ret_query, ("sp", "fs"), axis=0, tiled=True),
        lax.all_gather(w_ret_key, ("sp", "fs"), axis=0, tiled=True),
        lax.all_gather(w_ret_value, ("sp", "fs"), axis=0, tiled=True),
        lax.all_gather(w_q_down, ("sp", "fs"), axis=0, tiled=True),
        lax.all_gather(w_kv_down, ("sp", "fs"), axis=0, tiled=True),
        lax.all_gather(w_rope_key, ("sp", "fs"), axis=0, tiled=True),
        lax.all_gather(w_ret_out, ("sp", "fs"), axis=0, tiled=True),
        lax.all_gather(w_att_out, ("sp", "fs"), axis=0, tiled=True),
    )
    source = tokens[0].astype(jnp.float32)
    normed = rms_scale(source, norm_gain).astype(jnp.bfloat16)
    ret_cos, ret_sin = angle_tables(positions, RET_DIM)
    rope_cos, rope_sin = angle_tables(positions, ROPE_DIM)

    def project(weight):
        return jnp.dot(normed, weight, preferred_element_type=jnp.float32)

    part_q = project(full_q_down).astype(jnp.bfloat16)
    part_kv = project(full_kv_down).astype(jnp.bfloat16)
    lat_q_raw, lat_kv_raw = (
        lax.all_gather(part_q, "tp", axis=1, tiled=True),
        lax.all_gather(part_kv, "tp", axis=1, tiled=True),
    )
    retention_query = rotate(
        project(full_query).reshape(tok_rows, ret_local, RET_DIM),
        ret_cos[:, None],
        ret_sin[:, None],
    ).astype(jnp.bfloat16)
    retention_key = (
        rotate(
            project(full_key).reshape(tok_rows, ret_local, RET_DIM),
            ret_cos[:, None],
            ret_sin[:, None],
        )
        * RET_DIM ** (-0.5)
    ).astype(jnp.bfloat16)
    retention_value = project(full_value).reshape(tok_rows, ret_local, RET_DIM).astype(jnp.bfloat16)
    rope_key = rotate(project(full_rope), rope_cos, rope_sin).astype(jnp.bfloat16)
    log_rates = head_rate[:, None] + decay_shift[0]
    cumul = jnp.cumsum(log_rates, axis=1)
    offsets = jnp.arange(tok_rows, dtype=jnp.int32)
    lower_mask = offsets[None, :] <= offsets[:, None]
    decay_matrix = jnp.exp(
        jnp.where(lower_mask[None], cumul[:, :, None] - cumul[:, None, :], -jnp.inf)
    )
    block_score_grid = (
        jnp.einsum(
            "zgq,ugq->gzu", retention_query, retention_key, preferred_element_type=jnp.float32
        )
        * decay_matrix
    ).astype(jnp.bfloat16)
    inside_block_output = jnp.einsum(
        "vzs,svp->zvp", block_score_grid, retention_value, preferred_element_type=jnp.float32
    )
    block_output_sum = cumul[:, -1]
    weighted_values = (
        retention_key.astype(jnp.float32) * jnp.exp(block_output_sum[:, None] - cumul).T[:, :, None]
    )
    contribution = jnp.einsum(
        "uzj,uzv->zjv",
        weighted_values,
        retention_value.astype(jnp.float32),
        precision=TOP_PRECISION,
    )
    identity = (jnp.zeros_like(block_output_sum), jnp.zeros_like(contribution))
    before_log, before_state = prefix(
        (block_output_sum, contribution), "sp", chain_states, identity
    )
    q_latent = rms_scale(lat_q_raw.astype(jnp.float32), q_lat_gain).astype(jnp.bfloat16)
    kv_latent = rms_scale(lat_kv_raw.astype(jnp.float32), kv_lat_gain).astype(jnp.bfloat16)
    query_full = jnp.dot(q_latent, w_q_up, preferred_element_type=jnp.float32).reshape(
        tok_rows, att_local, NOPE_DIM + ROPE_DIM
    )
    query_nope = query_full[..., :NOPE_DIM].astype(jnp.bfloat16)
    query_rope = rotate(query_full[..., NOPE_DIM:], rope_cos[:, None], rope_sin[:, None]).astype(
        jnp.bfloat16
    )
    att_scale = (NOPE_DIM + ROPE_DIM) ** (-0.5)

    def attend(carry, key_nope, key_values, key_rope, start):
        running_max, running_sum, running_acc = carry
        key_count = key_rope.shape[0]
        score_matrix = (
            jnp.einsum("qhd,khd->hqk", query_nope, key_nope, preferred_element_type=jnp.float32)
            + jnp.einsum("qhd,kd->hqk", query_rope, key_rope, preferred_element_type=jnp.float32)
        ) * att_scale
        key_positions = start + jnp.arange(key_count, dtype=jnp.int32)
        allowed = key_positions[None, :] <= positions[:, None]
        masked = jnp.where(allowed[None], score_matrix, -jnp.inf)
        new_max = jnp.maximum(running_max, jnp.max(masked, axis=-1))
        safe_max = jnp.where(jnp.isfinite(new_max), new_max, 0.0)
        weights = jnp.exp(masked - safe_max[..., None])
        rescale = jnp.exp(running_max - safe_max)
        new_sum = running_sum * rescale + jnp.sum(weights, axis=-1)
        new_acc = running_acc * rescale[..., None] + jnp.einsum(
            "hqk,khd->hqd",
            weights.astype(jnp.bfloat16),
            key_values,
            preferred_element_type=jnp.float32,
        )
        return (new_max, new_sum, new_acc)

    def expand_attend(carry_in, lat_piece, rope_piece, start):
        wide = (
            jnp.dot(lat_piece, w_kv_up, preferred_element_type=jnp.float32)
            .astype(jnp.bfloat16)
            .reshape(rope_piece.shape[0], att_local, NOPE_DIM + VAL_DIM)
        )
        return attend(carry_in, wide[..., :NOPE_DIM], wide[..., NOPE_DIM:], rope_piece, start)

    empty = (
        jnp.full((att_local, tok_rows), -jnp.inf, jnp.float32),
        jnp.zeros((att_local, tok_rows), jnp.float32),
        jnp.zeros((att_local, tok_rows, VAL_DIM), jnp.float32),
    )
    groups = lax.axis_size("tp")
    kv_part = KV_LAT // groups
    rope_part = ROPE_DIM // groups
    my_group = lax.axis_index("tp")
    joined = jnp.concatenate(
        [
            lax.dynamic_slice_in_dim(kv_latent, my_group * kv_part, kv_part, 1),
            lax.dynamic_slice_in_dim(rope_key, my_group * rope_part, rope_part, 1),
        ],
        axis=1,
    )
    all_rows = lax.all_gather(joined, "sp", axis=0, tiled=True)
    complete = lax.all_gather(all_rows, "tp", axis=1, tiled=True)
    total_rows = complete.shape[0]
    grouped = complete.reshape(total_rows, groups, kv_part + rope_part)
    lat_all = grouped[:, :, :kv_part].reshape(total_rows, KV_LAT)
    rope_all = grouped[:, :, kv_part:].reshape(total_rows, ROPE_DIM)

    def visit(block_index, carry_in):
        start = block_index * tok_rows
        lat_piece = lax.dynamic_slice_in_dim(lat_all, start, tok_rows, 0)
        rope_piece = lax.dynamic_slice_in_dim(rope_all, start, tok_rows, 0)
        return expand_attend(carry_in, lat_piece, rope_piece, start)

    final = lax.fori_loop(0, lax.axis_index("sp") + 1, visit, empty)
    att_raw = jnp.transpose(final[2] / final[1][..., None], (1, 0, 2))
    att_out = (
        rms_scale(att_raw, att_norm_gain.reshape(att_local, VAL_DIM))
        .astype(jnp.bfloat16)
        .reshape(tok_rows, att_local * VAL_DIM)
    )
    entering = jnp.exp(before_log)[:, None, None] * start_state[0] + before_state
    carried_term = (
        jnp.einsum(
            "nhd,hde->nhe", retention_query.astype(jnp.float32), entering, precision=TOP_PRECISION
        )
        * jnp.exp(cumul).T[:, :, None]
    )
    ret_raw = inside_block_output + carried_term
    row_mean = jnp.mean(ret_raw, axis=-1, keepdims=True)
    centered = ret_raw - row_mean
    row_var = jnp.mean(centered * centered, axis=-1, keepdims=True)
    ret_out = (
        (centered * lax.rsqrt(row_var + EPSILON) * ret_norm_gain.reshape(ret_local, RET_DIM))
        .astype(jnp.bfloat16)
        .reshape(tok_rows, ret_local * RET_DIM)
    )
    contract = (((1,), (1,)), ((), ()))
    mixed = lax.psum_scatter(
        (
            lax.dot_general(ret_out, full_ret_out, contract, preferred_element_type=jnp.float32)
            + lax.dot_general(att_out, full_att_out, contract, preferred_element_type=jnp.float32)
        ).astype(jnp.bfloat16),
        "tp",
        scatter_dimension=0,
        tiled=True,
    )
    return mixed[None]


MESH = pl.DeviceIdType.MESH
WIDE = RET_DIM
CONTRACT = (((1,), (1,)), ((), ()))
GROUPS = ((0, 2), (2, 2), (4, 1), (5, 1))
FIRST, LATER = (0, 1), (2, 3)


def heads_fit(mesh, ret_local, sequences, q_wide, kv_wide, up_wide):
    sizes = mesh.shape
    return (
        sizes["sp"] == 4
        and sizes["fs"] == 4
        and sizes["tp"] == 2
        and ret_local == sizes["sp"]
        and sequences == 1
        and up_wide == 2 * (NOPE_DIM + ROPE_DIM) * ret_local
        and q_wide % 128 == 0
        and kv_wide % 128 == 0
        and q_wide + kv_wide + 2 * ROPE_DIM <= ret_local * WIDE
    )


def wave_tables(length, wide):
    half_wide = wide // 2
    powers = np.arange(half_wide, dtype=np.float32) * np.float32(2.0 / wide)
    inverse = np.power(np.float32(THETA_BASE), -powers).astype(np.float32)
    angles = np.arange(length, dtype=np.float32)[:, None] * inverse[None, :]
    return np.cos(angles), np.sin(angles)


def three_parts(x):
    high = x.astype(jnp.bfloat16)
    rest = x - high.astype(jnp.float32)
    middle = rest.astype(jnp.bfloat16)
    low = (rest - middle.astype(jnp.float32)).astype(jnp.bfloat16)
    return high, middle, low


def layer_kernel(
    n_sp,
    q_wide,
    kv_wide,
    tok_ref,
    lat_ref,
    wq_ref,
    wk_ref,
    wv_ref,
    wr_ref,
    wa_ref,
    shift_ref,
    rate_ref,
    gain_ref,
    qgain_ref,
    kvgain_ref,
    again_ref,
    rgain_ref,
    rcos_ref,
    rsin_ref,
    pcos_ref,
    psin_ref,
    qup_ref,
    kvup_ref,
    start_ref,
    out_ref,
    tok_all,
    w_all,
    shift_all,
    normed,
    acc,
    ret_q,
    ret_k,
    ret_v,
    lat_all,
    state,
    qn,
    qr,
    expanded,
    rope_key,
    kvup,
    qup,
    merged,
    own_sum,
    pair_out,
    pair_in,
    row_out,
    row_in,
    local_sem,
    z_send,
    z_recv,
    x_send,
    x_recv,
    y_send,
    y_recv,
    f_send,
    f_recv,
    m_send,
    m_recv,
    l_send,
    l_recv,
    l_relay,
    p_send,
    p_recv,
):
    z, f, t = lax.axis_index("sp"), lax.axis_index("fs"), lax.axis_index("tp")
    xn = f + 1 - 2 * (f % 2)
    yn = (f + 2) % 4
    other = 1 - t
    fs = 4
    rows = tok_ref.shape[0]
    half = rows // 2
    weights = (lat_ref, wq_ref, wk_ref, wv_ref, wr_ref, wa_ref)
    f32, bf16 = jnp.float32, jnp.bfloat16

    def remote(src, dst, send, recv, **where):
        return pltpu.make_async_remote_copy(
            src_ref=src,
            dst_ref=dst,
            send_sem=send,
            recv_sem=recv,
            device_id={"sp": z, "fs": f, "tp": t, **where},
            device_id_type=MESH,
        )

    barrier = pltpu.get_barrier_semaphore()
    peers = [{"sp": (z + d) % n_sp, "fs": f, "tp": t} for d in range(1, n_sp)]
    peers += [{"sp": z, "fs": xn, "tp": t}, {"sp": z, "fs": yn, "tp": t}]
    peers += [{"sp": z, "fs": f, "tp": other}]
    for peer in peers:
        pl.semaphore_signal(barrier, inc=1, device_id=peer, device_id_type=MESH)
    pl.semaphore_wait(barrier, len(peers))

    def piece(u, owner):
        return weights[u].at[:, pl.ds(pl.multiple_of(owner * WIDE, WIDE), WIDE)]

    def part(owner_z, owner_f, g):
        first, count = GROUPS[g]
        start = pl.multiple_of((owner_z * fs + owner_f) * rows, rows)
        return w_all.at[pl.ds(start, rows), pl.ds(first * WIDE, count * WIDE)]

    def unit(u):
        start = pl.multiple_of((z * fs + f) * rows, rows)
        return w_all.at[pl.ds(start, rows), pl.ds(u * WIDE, WIDE)]

    pending = []

    def go(copy):
        copy.start()
        pending.append(copy)
        return copy

    def owner(d):
        return (z + n_sp - d) % n_sp

    mine = pl.ds(pl.multiple_of(t * half, half), half)
    z_copies, x_copies, y_copies, f_copies = {}, {}, {}, {}

    def tok_part(origin):
        return tok_all.at[origin, mine]

    def lat_part(i):
        return lambda origin: lat_all.at[t, origin, pl.ds(i * rows, rows)]

    def direct(dest):
        near = (z - dest == 1) | (dest - z == 1)
        return near if dest in (0, n_sp - 1) else z != dest

    def line_copy(where, row, dest, src=None):
        return remote(
            where(z) if src is None else src,
            where(z),
            l_send.at[row, dest],
            l_recv.at[row, z],
            sp=dest,
        )

    def relay_copy(where, row, origin, dest):
        ref = where(origin)
        return remote(ref, ref, l_relay.at[row, origin], l_recv.at[row, origin], sp=dest)

    def pair_copy(where, row, origin):
        ref = where(origin)
        return remote(ref, ref, p_send.at[row, origin], p_recv.at[row, origin], tp=other)

    def line_start(where, row, src=None, pair=True):
        for dest in range(n_sp):
            pl.when(direct(dest))(lambda dest=dest: line_copy(where, row, dest, src).start())
        if pair:
            for origin in range(n_sp):
                pl.when(origin == z)(
                    lambda origin=origin: pair_copy(where, row, origin).start()
                )

    def passes_on(origin):
        if origin < n_sp // 2:
            return z == n_sp - 2, n_sp - 1
        return z == 1, 0

    def line_pass(where, row):
        for origin in range(n_sp):

            @pl.when(origin != z)
            def _(origin=origin):
                relay_copy(where, row, origin, 0).wait_recv()
                should, dest = passes_on(origin)
                pl.when(should)(lambda: relay_copy(where, row, origin, dest).start())
                pair_copy(where, row, origin).start()

    def pair_arrive(where, row, own):
        for origin in range(n_sp):
            if own:
                pair_copy(where, row, origin).wait_recv()
            else:
                pl.when(origin != z)(
                    lambda origin=origin: pair_copy(where, row, origin).wait_recv()
                )

    def line_drain(where, row, own):
        for other_z in range(n_sp):
            pl.when(direct(other_z))(
                lambda dest=other_z: line_copy(where, row, dest).wait_send()
            )
            if own:
                pair_copy(where, row, other_z).wait_send()

            @pl.when(other_z != z)
            def _(origin=other_z):
                should, dest = passes_on(origin)
                pl.when(should)(lambda: relay_copy(where, row, origin, dest).wait_send())
                if not own:
                    pair_copy(where, row, origin).wait_send()

    line_start(tok_part, 0, tok_ref.at[mine], pair=False)
    for d in range(1, n_sp):
        to = (z + d) % n_sp
        go(remote(shift_ref, shift_all.at[z], m_send.at[2, d], m_recv.at[2, d], sp=to))
    shift_copies = list(pending)
    pending.clear()
    locals_ = []
    for u in range(6):
        copy = pltpu.make_async_copy(piece(u, z), unit(u), local_sem.at[u])
        copy.start()
        locals_.append(copy)
    own_tok = pltpu.make_async_copy(tok_ref, tok_all.at[z], local_sem.at[6])
    own_tok.start()
    own_shift = pltpu.make_async_copy(shift_ref, shift_all.at[z], local_sem.at[7])
    own_shift.start()
    att_wide = kvup.shape[1]
    own_kvup = pltpu.make_async_copy(
        kvup_ref.at[:, pl.ds(pl.multiple_of(z * att_wide, att_wide), att_wide)],
        kvup,
        local_sem.at[8],
    )
    own_kvup.start()
    up_wide = qup.shape[1]
    own_qup = pltpu.make_async_copy(
        qup_ref.at[:, pl.ds(pl.multiple_of(z * up_wide, up_wide), up_wide)],
        qup,
        local_sem.at[10],
    )
    own_qup.start()
    own_state = pltpu.make_async_copy(start_ref.at[z], state, local_sem.at[9])
    own_state.start()
    for group in (FIRST, LATER):
        for d in range(1, n_sp):
            to = (z + d) % n_sp
            for g in group:
                for u in range(GROUPS[g][0], sum(GROUPS[g])):
                    z_copies[d, u] = remote(
                        piece(u, to), unit(u), z_send.at[d, u], z_recv.at[d, u], sp=to
                    )
                    z_copies[d, u].start()

    def spread(d, group):
        for g in group:
            for u in range(GROUPS[g][0], sum(GROUPS[g])):
                if d == 0:
                    locals_[u].wait()
                else:
                    z_copies[d, u].wait_recv()
            ref = part(owner(d), f, g)
            x_copies[d, g] = remote(ref, ref, x_send.at[d, g], x_recv.at[d, g], fs=xn)
            y_copies[d, g] = remote(ref, ref, y_send.at[d, g], y_recv.at[d, g], fs=yn)
            x_copies[d, g].start()
            y_copies[d, g].start()

    def relay(d, group):
        for g in group:
            if g % 2 == 0:
                x_copies[d, g].wait_recv()
                ref, to = part(owner(d), xn, g), yn
            else:
                y_copies[d, g].wait_recv()
                ref, to = part(owner(d), yn, g), xn
            f_copies[d, g] = remote(ref, ref, f_send.at[d, g], f_recv.at[d, g], fs=to)
            f_copies[d, g].start()

    def arrive(d, group):
        for g in group:
            if g % 2 == 0:
                y_copies[d, g].wait_recv()
            else:
                x_copies[d, g].wait_recv()
            f_copies[d, g].wait_recv()

    def at(i):
        if isinstance(i, int):
            return slice(i * rows, (i + 1) * rows)
        return pl.ds(pl.multiple_of(i * rows, rows), rows)

    def norm_block(i):
        x = tok_all[i].astype(f32)
        scaled = x * lax.rsqrt(jnp.mean(x * x, axis=-1, keepdims=True) + EPSILON)
        normed[at(i), :] = (scaled * gain_ref[...]).astype(bf16)

    spread(0, FIRST)
    own_tok.wait()
    norm_block(z)
    line_pass(tok_part, 0)
    for d in range(1, n_sp):
        spread(d, FIRST)
        relay(d - 1, FIRST)
        if d == 1:
            pair_arrive(tok_part, 0, False)
        norm_block(owner(d))
    relay(n_sp - 1, FIRST)
    spread(0, LATER)
    depth = fs * rows
    for d in range(n_sp):
        arrive(d, FIRST)
        begin = pl.multiple_of(owner(d) * depth, depth)

        def multiply(i, carry, d=d, begin=begin):
            columns = pl.ds(pl.multiple_of(i * WIDE, WIDE), WIDE)
            got = jnp.dot(
                normed[:, pl.ds(begin, depth)],
                w_all[pl.ds(begin, depth), columns],
                preferred_element_type=f32,
            )
            if d == 0:
                acc[:, columns] = got
            else:
                acc[:, columns] += got
            return carry

        lax.fori_loop(0, 4, multiply, 0)

    rope_index = (q_wide + kv_wide) // WIDE
    rope_lane = (q_wide + kv_wide) % WIDE
    rd = RET_DIM // 2

    def finish_lat(i, carry):
        raw = acc[at(i), :WIDE]
        pair = raw[:, rope_lane : rope_lane + 2 * ROPE_DIM]
        turned = pair * pcos_ref[at(i), :] + pltpu.roll(pair, ROPE_DIM, 1) * psin_ref[at(i), :]
        lane = lax.broadcasted_iota(jnp.int32, turned.shape, 1)
        turned = jnp.where(lane < ROPE_DIM, turned, pltpu.roll(turned, ROPE_DIM, 1))
        pieces = [raw[:, :rope_lane]] if rope_lane else []
        pieces.append(jnp.where(z == rope_index, turned, pair))
        if rope_lane + 2 * ROPE_DIM < WIDE:
            pieces.append(raw[:, rope_lane + 2 * ROPE_DIM :])
        lat_all[t, z, at(i), :] = jnp.concatenate(pieces, axis=1).astype(bf16)
        return carry

    for i in range(n_sp):
        finish_lat(i, 0)
        line_start(lat_part(i), i + 1)

    def finish_ret(i, carry):
        cosine, sine = rcos_ref[at(i), :], rsin_ref[at(i), :]
        for dst, base, factor in ((ret_q, WIDE, 1.0), (ret_k, 2 * WIDE, RET_DIM ** (-0.5))):
            a, b = acc[at(i), base : base + rd], acc[at(i), base + rd : base + WIDE]
            dst[at(i), :rd] = ((a * cosine - b * sine) * factor).astype(bf16)
            dst[at(i), rd:] = ((b * cosine + a * sine) * factor).astype(bf16)
        ret_v[at(i), :] = acc[at(i), 3 * WIDE :].astype(bf16)
        return carry

    lax.fori_loop(0, n_sp, finish_ret, 0)

    for copy in shift_copies:
        copy.wait()
    own_shift.wait()
    own_state.wait()
    r_iota = lax.broadcasted_iota(jnp.int32, (rows, rows), 0)
    c_iota = lax.broadcasted_iota(jnp.int32, (rows, rows), 1)

    def retention(b):
        rates = shift_all[b]
        pick = lax.broadcasted_iota(jnp.int32, rates.shape, 0) == z
        chosen = lax.broadcasted_iota(jnp.int32, rate_ref.shape, 1) == z
        rate = jnp.sum(jnp.where(chosen, rate_ref[...], 0.0), axis=1, keepdims=True)
        row = jnp.sum(jnp.where(pick, rates, 0.0), axis=0, keepdims=True) + rate
        column = jnp.sum(jnp.where(r_iota == c_iota, row, 0.0), axis=1, keepdims=True)
        c_col = jnp.sum(jnp.where(c_iota <= r_iota, row, 0.0), axis=1, keepdims=True)
        c_row = jnp.sum(jnp.where(r_iota <= c_iota, column, 0.0), axis=0, keepdims=True)
        last = jnp.sum(row, axis=1, keepdims=True)
        decay = jnp.exp(jnp.where(c_iota <= r_iota, c_col - c_row, -jnp.inf))
        block = slice(b * rows, (b + 1) * rows)
        q, k, v = ret_q[block, :], ret_k[block, :], ret_v[block, :]
        scores = lax.dot_general(q, k, CONTRACT, preferred_element_type=f32) * decay
        raw = jnp.dot(scores.astype(bf16), v, preferred_element_type=f32)
        carried = sum(
            jnp.dot(q, s, preferred_element_type=f32) for s in three_parts(state[...])
        )
        raw = raw + carried * jnp.exp(c_col)
        if b < n_sp - 1:
            weighted = k.astype(f32) * jnp.exp(last - c_col)
            added = sum(
                lax.dot_general(w, v, (((0,), (0,)), ((), ())), preferred_element_type=f32)
                for w in three_parts(weighted)
            )
            state[...] = jnp.exp(last) * state[...] + added
        centered = raw - jnp.mean(raw, axis=-1, keepdims=True)
        variance = jnp.mean(centered * centered, axis=-1, keepdims=True)
        merged[block, :WIDE] = (centered * lax.rsqrt(variance + EPSILON) * rgain_ref[z]).astype(
            bf16
        )

    for b in range(n_sp):
        if b:
            spread(b, LATER)
            relay(b - 1, LATER)
        line_pass(lat_part(b), b + 1)
        retention(b)
    relay(n_sp - 1, LATER)
    own_kvup.wait()
    own_qup.wait()

    def chunks(first, count):
        found = []
        for core in range(2):
            for j in range(count // 128):
                lane = first + j * 128
                found.append((core, lane // WIDE, lane % WIDE))
        return found

    q_chunks, kv_chunks = chunks(0, q_wide), chunks(q_wide, kv_wide)
    rope_at = (rope_index, rope_lane)
    att_heads = att_wide // (NOPE_DIM + VAL_DIM)
    nope = att_heads * NOPE_DIM
    turn = att_heads * ROPE_DIM

    def expand(i, carry):
        def latent(found, gain):
            x = jnp.concatenate(
                [lat_all[c, s, at(i), lane : lane + 128] for c, s, lane in found], axis=1
            ).astype(f32)
            scaled = x * lax.rsqrt(jnp.mean(x * x, axis=-1, keepdims=True) + EPSILON)
            return (scaled * gain[...]).astype(bf16)

        query = jnp.dot(latent(q_chunks, qgain_ref), qup[...], preferred_element_type=f32)
        first, middle, end = query[:, :128], query[:, 128:256], query[:, 256:]
        lane = lax.broadcasted_iota(jnp.int32, first.shape, 1)
        second = jnp.where(
            lane < ROPE_DIM, pltpu.roll(middle, ROPE_DIM, 1), pltpu.roll(end, ROPE_DIM, 1)
        )
        pair = jnp.where(lane < ROPE_DIM, middle, end)
        quarter = ROPE_DIM // 2
        swapped = jnp.where(
            lane % ROPE_DIM < quarter,
            pltpu.roll(pair, 2 * ROPE_DIM - quarter, 1),
            pltpu.roll(pair, quarter, 1),
        )
        qn[at(i), :NOPE_DIM] = first.astype(bf16)
        qn[at(i), NOPE_DIM:] = second.astype(bf16)
        qr[at(i), :] = (pair * pcos_ref[at(i), :] + swapped * psin_ref[at(i), :]).astype(bf16)
        expanded[at(i), :] = jnp.dot(
            latent(kv_chunks, kvgain_ref), kvup[...], preferred_element_type=f32
        ).astype(bf16)
        rope_key[at(i), :] = lat_all[0, rope_at[0], at(i), rope_at[1] : rope_at[1] + 128]
        return carry

    for i in range(n_sp):
        pair_arrive(lat_part(i), i + 1, True)
        expand(i, 0)
    for d in range(n_sp):
        arrive(d, LATER)
    pair_copies = {}

    def row_copy(b, origin):
        return remote(row_out.at[b], row_in.at[origin], m_send.at[6, b], m_recv.at[6, origin], sp=b)

    def project_out(b):
        got = lax.dot_general(
            merged[b * rows : (b + 1) * rows, :],
            w_all[:, 4 * WIDE :],
            CONTRACT,
            preferred_element_type=f32,
        )
        front, back = got[:half, :], got[half:, :]
        pair_out[b] = jnp.where(t == 0, back, front).astype(bf16)
        pair_copies[b] = remote(
            pair_out.at[b], pair_in.at[b], m_send.at[5, b], m_recv.at[5, b], tp=other
        )
        pair_copies[b].start()
        own_sum[b] = jnp.where(t == 0, front, back)

    def send_rows(b):
        pair_copies[b].wait_recv()
        total = own_sum[b] + pair_in[b].astype(f32)
        own_sum[b] = total

        @pl.when(z != b)
        def _():
            row_out[b] = total.astype(bf16)
            row_copy(b, z).start()

    scale = (NOPE_DIM + ROPE_DIM) ** (-0.5)
    order = (0, n_sp - 1) + tuple(range(1, n_sp - 1))
    for step, b in enumerate(order):
        seen = (b + 1) * rows
        block = slice(b * rows, seen)
        q_at = lax.broadcasted_iota(jnp.int32, (rows, seen), 0) + b * rows
        k_at = lax.broadcasted_iota(jnp.int32, (rows, seen), 1)
        for h in range(att_heads):
            base = h * (NOPE_DIM + VAL_DIM)
            turned = qr[block, :]
            lane = lax.broadcasted_iota(jnp.int32, turned.shape, 1)
            turned = jnp.where(lane // ROPE_DIM == h, turned, jnp.zeros_like(turned))
            s = lax.dot_general(
                qn[block, h * NOPE_DIM : (h + 1) * NOPE_DIM],
                expanded[:seen, base : base + NOPE_DIM],
                CONTRACT,
                preferred_element_type=f32,
            ) + lax.dot_general(
                turned, rope_key[:seen, :], CONTRACT, preferred_element_type=f32
            )
            s = jnp.where(k_at <= q_at, s * scale, -jnp.inf)
            p = jnp.exp(s - jnp.max(s, axis=-1, keepdims=True))
            raw = jnp.dot(
                p.astype(bf16),
                expanded[:seen, base + NOPE_DIM : base + NOPE_DIM + VAL_DIM],
                preferred_element_type=f32,
            ) / jnp.sum(p, axis=-1, keepdims=True)
            scaled = raw * lax.rsqrt(jnp.mean(raw * raw, axis=-1, keepdims=True) + EPSILON)
            gain = again_ref[z][:, h * VAL_DIM : (h + 1) * VAL_DIM]
            merged[block, WIDE + h * VAL_DIM : WIDE + (h + 1) * VAL_DIM] = (
                scaled * gain
            ).astype(bf16)

        project_out(b)
        if step:
            send_rows(order[step - 1])
    send_rows(order[-1])
    total = own_sum[z]
    for d in range(1, n_sp):
        row_copy(0, owner(d)).wait_recv()
        total = total + row_in[owner(d)].astype(f32)
    out_ref[...] = total.astype(bf16)

    for group in (z_copies, x_copies, y_copies, f_copies, pair_copies):
        for copy in group.values():
            copy.wait_send()
    line_drain(tok_part, 0, False)
    for i in range(n_sp):
        line_drain(lat_part(i), i + 1, True)
    for b in range(n_sp):
        pl.when(z != b)(lambda b=b: row_copy(b, z).wait_send())


def heads_plan(
    tokens,
    norm_gain,
    w_ret_query,
    w_ret_key,
    w_ret_value,
    w_q_down,
    w_kv_down,
    w_rope_key,
    w_q_up,
    w_kv_up,
    q_lat_gain,
    kv_lat_gain,
    att_norm_gain,
    ret_norm_gain,
    w_ret_out,
    w_att_out,
    head_rate,
    decay_shift,
    start_state,
):
    n_sp = lax.axis_size("sp")
    rows, width = tokens.shape[1:]
    length = n_sp * rows
    q_wide, kv_wide = w_q_down.shape[1], w_kv_down.shape[1]
    rope_half = ROPE_DIM // 2
    w_rows = w_q_down.shape[0]
    att_heads = w_q_up.shape[1] // (NOPE_DIM + ROPE_DIM) // n_sp

    def swap(x):
        return jnp.concatenate([x[..., rope_half:], x[..., :rope_half]], axis=-1)

    lat = jnp.concatenate([w_q_down, w_kv_down, w_rope_key, swap(w_rope_key)], axis=1)
    lat = jnp.pad(lat, ((0, 0), (0, n_sp * WIDE - lat.shape[1])))
    ret_cos, ret_sin = wave_tables(length, RET_DIM)
    rope_cos, rope_sin = wave_tables(length, ROPE_DIM)
    pair_cos = np.concatenate([rope_cos] * 4, axis=1)
    pair_sin = np.concatenate([-rope_sin, rope_sin] * 2, axis=1)
    dma = pltpu.SemaphoreType.DMA
    vmem = pltpu.VMEM
    f32, bf16 = jnp.float32, jnp.bfloat16
    half = rows // 2
    out_wide = 4 * n_sp * w_rows
    any_spec = pl.BlockSpec(memory_space=pl.ANY)
    vmem_spec = pl.BlockSpec(memory_space=pltpu.VMEM)
    mixed = pl.pallas_call(
        functools.partial(layer_kernel, n_sp, q_wide, kv_wide),
        out_shape=jax.ShapeDtypeStruct((half, out_wide), bf16),
        in_specs=[any_spec] * 8 + [vmem_spec] * 10 + [any_spec] * 3,
        out_specs=vmem_spec,
        scratch_shapes=[
            vmem((n_sp, rows, width), bf16),
            vmem((n_sp * 4 * w_rows, 6 * WIDE), bf16),
            vmem((n_sp,) + decay_shift.shape[1:], f32),
            vmem((length, width), bf16),
            vmem((length, 4 * WIDE), f32),
            vmem((length, WIDE), bf16),
            vmem((length, WIDE), bf16),
            vmem((length, WIDE), bf16),
            vmem((2, n_sp, length, WIDE), bf16),
            vmem((RET_DIM, RET_DIM), f32),
            vmem((length, att_heads * NOPE_DIM), bf16),
            vmem((length, att_heads * ROPE_DIM), bf16),
            vmem((length, att_heads * (NOPE_DIM + VAL_DIM)), bf16),
            vmem((length, 2 * ROPE_DIM), bf16),
            vmem((w_kv_up.shape[0], att_heads * (NOPE_DIM + VAL_DIM)), bf16),
            vmem((w_q_up.shape[0], att_heads * (NOPE_DIM + ROPE_DIM)), bf16),
            vmem((length, WIDE + att_heads * VAL_DIM), bf16),
            vmem((n_sp, half, out_wide), f32),
            vmem((n_sp, half, out_wide), bf16),
            vmem((n_sp, half, out_wide), bf16),
            vmem((n_sp, half, out_wide), bf16),
            vmem((n_sp, half, out_wide), bf16),
            dma((11,)),
            dma((n_sp, 6)),
            dma((n_sp, 6)),
            dma((n_sp, 4)),
            dma((n_sp, 4)),
            dma((n_sp, 4)),
            dma((n_sp, 4)),
            dma((n_sp, 4)),
            dma((n_sp, 4)),
            dma((7, n_sp)),
            dma((7, n_sp)),
            dma((n_sp + 1, n_sp)),
            dma((n_sp + 1, n_sp)),
            dma((n_sp + 1, n_sp)),
            dma((n_sp + 1, n_sp)),
            dma((n_sp + 1, n_sp)),
        ],
        compiler_params=pltpu.CompilerParams(
            collective_id=0, has_side_effects=True, vmem_limit_bytes=62 * 1024 * 1024
        ),
    )(
        tokens[0],
        lat,
        w_ret_query,
        w_ret_key,
        w_ret_value,
        w_ret_out,
        w_att_out,
        decay_shift[0],
        head_rate[None],
        norm_gain[None],
        q_lat_gain[None],
        kv_lat_gain[None],
        att_norm_gain.reshape(n_sp, 1, -1),
        ret_norm_gain.reshape(n_sp, 1, -1),
        ret_cos,
        ret_sin,
        pair_cos,
        pair_sin,
        w_q_up,
        w_kv_up,
        start_state[0],
    )
    return mixed[None]


def solution(mesh):
    placed = (
        P("fs", "sp", None),
        P(),
        P(("sp", "fs"), "tp"),
        P(("sp", "fs"), "tp"),
        P(("sp", "fs"), "tp"),
        P(("sp", "fs"), "tp"),
        P(("sp", "fs"), "tp"),
        P(("sp", "fs"), None),
        P(None, "tp"),
        P(None, "tp"),
        P(),
        P(),
        P("tp"),
        P("tp"),
        P(("sp", "fs"), "tp"),
        P(("sp", "fs"), "tp"),
        P("tp"),
        P("fs", "tp", "sp"),
        P("fs", "tp", None, None),
    )

    def pick(*args):
        if heads_fit(
            mesh, args[16].shape[0], args[0].shape[0], args[5].shape[1], args[6].shape[1], args[8].shape[1]
        ):
            return heads_plan(*args)
        return rows_plan(*args)

    return jax.shard_map(
        pick,
        mesh=mesh,
        in_specs=placed,
        out_specs=P("fs", ("sp", "tp"), None),
        check_vma=False,
    )
```
